32 devices in a mesh: sp: 8 (over z, y), tp: 4 (over x, core).
Axes of the slice: x: 2, y: 2, z: 4, core: 2. Of those that a mesh axis runs over, the one named last changes fastest.
Arguments:
- layer_input: bfloat16 [4096, 2048], P('sp'), may hold values from -6 to 6
- out_cot: bfloat16 [4096, 2048], P('sp'), may hold values from -6 to 6
- expert_ids: int32 [4096, 2], P('sp'), may hold values from 0 to 7, all different within a row; in each aligned block of 512 rows (0 to 511, 512 to 1023, ...) at most 160 rows name the same one
- route_weight: float32 [4096, 2], P('sp'), may hold values from 0.1 to 1
- w_gate: bfloat16 [8, 2048, 1024], P('sp', None, 'tp'), may hold values from -0.125 to 0.125
- w_up: bfloat16 [8, 2048, 1024], P('sp', None, 'tp'), may hold values from -0.125 to 0.125
- w_down: bfloat16 [8, 1024, 2048], P('sp', 'tp'), may hold values from -0.1875 to 0.1875
- out_proj: bfloat16 [2048, 1024], P(None, 'tp'), may hold values from -0.1875 to 0.1875
- rec_input: bfloat16 [4096, 1024], P('sp', 'tp'), may hold values from -6 to 6
- gate_input: bfloat16 [4096, 1024], P('sp', 'tp'), may hold values from -6 to 6
- prev_state: float32 [4096, 1024], P('sp', 'tp'), may hold values from -6 to 6
- decay_param: float32 [1024], replicated, may hold values from 4 to 20
- extra_decay: float32 [8, 4096], P('tp', 'sp'), may hold values from -3 to 0, as said below
- gate_a_w: bfloat16 [8, 128, 128], replicated, may hold values from -0.5 to 0.5
- gate_i_w: bfloat16 [8, 128, 128], replicated, may hold values from -0.5 to 0.5
Outputs:
- grad_gate: float32 [8, 2048, 1024], P('sp', None, 'tp')
- grad_up: float32 [8, 2048, 1024], P('sp', None, 'tp')
- grad_down: float32 [8, 1024, 2048], P('sp', 'tp')
- grad_out_proj: float32 [2048, 1024], P('sp', 'tp')
- rec_input_grad: bfloat16 [4096, 1024], P('sp', 'tp')
- gate_input_grad: bfloat16 [4096, 1024], P('sp', 'tp')
The draws below stay inside these ranges and needn't reach their ends.
Inputs may be any that keep to these rules, and one draw needn't show every extreme that they name: `expert_ids`: each row names 2 different experts; among the slots of the tokens of one sp index (aligned blocks of 512 rows) no expert is named more than 160 times, and in every draw some expert is named exactly 160 times in some block. `extra_decay`: every entry is at most -0.05 / 4096.
All inputs are finite; a program needn't handle non-finite values.
Results may differ from the reference program's by a relative error of at most 0.017.
Values may be sent and summed in bfloat16 or wider, within the bound.
A program may use at most 128 MiB of HBM per device.

```python
import math
import jax
import jax.numpy as jnp
import numpy as np
from jax import lax

D = 2048
FF = 1024
RECURRENT_HEADS = 8
HEAD_DIM = 128
TOP = 2
TOK_DEV = 512
D_LRU = 1024
EXPERTS = 8
TOKENS = 4096
CAP = 160
EXP_ROWS = 1280
N_SP = 8
N_TP = 4


def draw_decay_param(key, part):
    head_key, rate_random_key = jax.random.split(jax.random.fold_in(key, 11))
    picks = jax.random.randint(head_key, (RECURRENT_HEADS,), 0, 10)
    quick = picks < 5
    unit = jax.random.uniform(rate_random_key, (RECURRENT_HEADS, HEAD_DIM), jnp.float32)
    quick_rate = 0.0025 * 4.0 ** unit
    slow_rate = 0.02 / TOKENS * 5.0 ** unit
    rate = jnp.where(quick[:, None], quick_rate, slow_rate).reshape(RECURRENT_HEADS * HEAD_DIM)
    return (-jnp.log(jnp.expm1(rate))).astype(jnp.float32)


def draw_extra_decay(key, part):
    rate_random_key, spike_random_key, placement_random_key = jax.random.split(jax.random.fold_in(key, 23), 3)
    blocks = TOKENS // TOK_DEV
    unit = jax.random.uniform(rate_random_key, (RECURRENT_HEADS, blocks), jnp.float32)
    block_rate = 0.1 / TOKENS * 10.0 ** unit
    token_wise = jnp.repeat(block_rate, TOK_DEV, axis=1)
    spots = jax.random.randint(placement_random_key, (RECURRENT_HEADS, 3), 0, TOKENS)
    retained_mask = jax.random.uniform(spike_random_key, (RECURRENT_HEADS, 3), jnp.float32, 0.5, 0.8)
    match_count = (spots[:, :, None] == jnp.arange(TOKENS, dtype=jnp.int32)[None, None, :]).astype(jnp.float32)
    spike_amount = jnp.sum(match_count * jnp.log(retained_mask)[:, :, None], axis=1)
    return (spike_amount - token_wise).astype(jnp.float32)


def raised(values, stream_key, source, target, blocks, factor):
    def block_of(position):
        return (jnp.arange(values.shape[position]) // (values.shape[position] // blocks)).reshape((-1,) + (1,) * (values.ndim - 1 - position))

    one_side = jax.random.permutation(stream_key, blocks)[block_of(target)]
    far = (block_of(target) + blocks // 2) % blocks
    return jnp.where((block_of(source) == one_side) | (block_of(source) == far), factor * values, values)


def shard_levels(stream_key, shape, pieces, low, high):
    loudness = 1.0
    for axis_at, parts in pieces:
        steps = jax.random.uniform(jax.random.fold_in(jax.random.fold_in(stream_key, 6), axis_at), (parts,), jnp.float32, low / len(pieces), high / len(pieces))
        loudness = loudness * jnp.repeat(jnp.exp(steps), shape[axis_at] // parts).reshape((-1,) + (1,) * (len(shape) - 1 - axis_at))
    return loudness


def deal_out(stream_key, own, number, rows, amount, top, reach, skew):
    ranking = jax.random.permutation(stream_key, amount)
    crowded, usual = portions_of(amount, rows * top, reach, skew, True), portions_of(amount, rows * top, reach, skew, False)
    places = jnp.arange(amount)

    def named(lengths, turn):
        used = int((lengths > 0).sum())
        fixed = max(1, used // 4)
        shifted = fixed + (places - fixed + turn * (used - fixed)) % max(1, amount - fixed)
        return jnp.zeros((amount,), jnp.int32).at[ranking[jnp.where(places < fixed, places, shifted)]].set(jnp.asarray(lengths, jnp.int32))

    lengths = jnp.where(number % 4 == 0, named(crowded, number // 4), named(usual, number - number // 4 - 1))
    mixed = jax.random.permutation(jax.random.fold_in(own, 3), amount)
    giver, sink = mixed[0:amount // 2 * 2:2], mixed[1:amount // 2 * 2:2]
    room = jnp.minimum(lengths[giver] - 1, reach - lengths[sink]) // 2
    room = jnp.where((giver == ranking[0]) | (sink == ranking[0]) | (lengths[sink] == 0), 0, jnp.maximum(room, 0))
    shifted = jax.random.randint(jax.random.fold_in(own, 4), (amount // 2,), 0, 1 << 20) % (room + 1)
    lengths = lengths.at[giver].add(-shifted).at[sink].add(shifted)
    items = jnp.searchsorted(jnp.cumsum(lengths), jnp.arange(rows * top), side="right").astype(jnp.int32)
    table = items.reshape(top, rows).T
    table = table[jax.random.permutation(jax.random.fold_in(own, 1), rows)]
    turn = jax.random.randint(jax.random.fold_in(own, 2), (rows, 1), 0, top)
    return jnp.take_along_axis(table, (jnp.arange(top)[None, :] + turn) % top, axis=1)


def portions_of(amount, total, limit, lean, full):
    loads = [(1 << 20) // math.isqrt(grade ** lean) + 1 for grade in range(1, amount + 1)]
    largest = limit if full else min(limit, max(-(-total // amount), total * loads[0] // sum(loads)))
    least = 1 if total - largest >= amount - 1 else 0
    holding, rest = [largest] + [least] * (amount - 1), total - largest - least * (amount - 1)
    while rest > 0:
        candidates = [i for i in range(1, amount) if holding[i] < largest] or [i for i in range(1, amount) if holding[i] < limit]
        pool, left = sum([loads[i] for i in candidates]), rest
        for i in candidates:
            extra = min(limit - holding[i], max(1, left * loads[i] // pool), rest)
            holding[i] = holding[i] + extra
            rest = rest - extra
    return np.array(holding)


def centred(key, dims, width, limit, cuts=(), kind=jnp.bfloat16):
    entries = width * jax.random.normal(key, dims, jnp.float32)
    if cuts:
        entries = entries * shard_levels(key, dims, cuts, -0.22, 0.18)
    return jnp.clip(entries, -limit, limit).astype(kind)


def noise_with(rng, extent, width, most, cuts, heavy, kind=jnp.bfloat16):
    entries = width * jax.random.normal(rng, extent, jnp.float32)
    if cuts:
        entries = entries * shard_levels(rng, extent, cuts, -0.22, 0.18)
    return jnp.clip(raised(entries, jax.random.fold_in(rng, 3), *heavy), -most, most).astype(kind)


def setup_inputs(seed: int = 0) -> dict:
    seeds = jax.random.split(jax.random.key(seed), 16)
    layer_input = centred(seeds[0], (TOKENS, D), 1.0, 6.0, ((0, 8),))
    out_cot = noise_with(seeds[1], (TOKENS, D), 1.0, 6.0, ((0, 8),), (0, 1, 8, 2.0))
    expert_ids_keys = jax.random.split(jax.random.fold_in(seeds[2], 1), TOKENS // TOK_DEV)
    expert_ids_turns = jax.random.permutation(jax.random.fold_in(seeds[2], 3), TOKENS // TOK_DEV)
    expert_ids = jax.vmap(lambda own, number: deal_out(jax.random.fold_in(seeds[2], 2), own, number, TOK_DEV, EXPERTS, TOP, CAP, 1))(expert_ids_keys, expert_ids_turns).reshape((TOKENS, TOP))
    route_weight = jnp.clip(0.1 + 0.9 * jax.random.uniform(seeds[3], (TOKENS, TOP), jnp.float32) ** shard_levels(seeds[3], (TOKENS, TOP), ((0, 8),), -0.2, 0.2), 0.1, 1.0)
    w_gate = centred(seeds[4], (EXPERTS, D, FF), D ** -0.5, 0.125, ((0, 8), (2, 4)))
    w_up = centred(seeds[5], (EXPERTS, D, FF), D ** -0.5, 0.125, ((0, 8), (2, 4)))
    w_down = centred(seeds[6], (EXPERTS, FF, D), FF ** -0.5, 0.1875, ((0, 8), (1, 4)))
    out_proj = centred(seeds[7], (D, D_LRU), D_LRU ** -0.5, 0.1875, ((1, 4),))
    rec_input = centred(seeds[8], (TOKENS, D_LRU), 1.0, 6.0, ((0, 8), (1, 4)))
    gate_input = centred(seeds[9], (TOKENS, D_LRU), 1.0, 6.0, ((0, 8), (1, 4)))
    prev_state = centred(seeds[10], (TOKENS, D_LRU), 1.0, 6.0, ((0, 8), (1, 4)), jnp.float32)
    decay_param = draw_decay_param(jax.random.fold_in(seeds[15], 71), 0)
    extra_decay = draw_extra_decay(jax.random.fold_in(seeds[15], 71), 0)
    gate_a_w = centred(seeds[13], (RECURRENT_HEADS, HEAD_DIM, HEAD_DIM), HEAD_DIM ** -0.5, 0.5)
    gate_i_w = centred(seeds[14], (RECURRENT_HEADS, HEAD_DIM, HEAD_DIM), HEAD_DIM ** -0.5, 0.5)
    return {"layer_input": layer_input, "out_cot": out_cot, "expert_ids": expert_ids, "route_weight": route_weight, "w_gate": w_gate, "w_up": w_up, "w_down": w_down, "out_proj": out_proj, "rec_input": rec_input, "gate_input": gate_input, "prev_state": prev_state, "decay_param": decay_param, "extra_decay": extra_decay, "gate_a_w": gate_a_w, "gate_i_w": gate_i_w}


gelu_scale = 0.7978845608028654
gelu_cubic = 0.044715
decay_factor = 8.0

def gelu_pair(values_in):
    inner = gelu_scale * (values_in + gelu_cubic * values_in * values_in * values_in)
    bend = jnp.tanh(inner)
    active = 0.5 * values_in * (1.0 + bend)
    slope = 0.5 * (1.0 + bend) + 0.5 * values_in * (1.0 - bend * bend) * gelu_scale * (1.0 + 3.0 * gelu_cubic * values_in * values_in)
    return (active, slope)

def head_product(row_block, weights, backward):
    blocks = row_block.astype(jnp.float32).reshape(row_block.shape[0], RECURRENT_HEADS, HEAD_DIM)
    wide = weights.astype(jnp.float32)
    if backward:
        result = jnp.einsum('nhe,hde->nhd', blocks, wide)
    else:
        result = jnp.einsum('nhd,hde->nhe', blocks, wide)
    return result.reshape(row_block.shape[0], RECURRENT_HEADS * HEAD_DIM)

def chain_link(earlier, later):
    return (earlier[0] * later[0], later[0] * earlier[1] + later[1])

def expert_backward(operands):
    row_block, cot_block, gate_w, up_w, down_w = operands
    gate_pre = jnp.dot(row_block, gate_w, preferred_element_type=jnp.float32)
    up_pre = jnp.dot(row_block, up_w, preferred_element_type=jnp.float32)
    sigma = jax.nn.sigmoid(gate_pre)
    swish = gate_pre * sigma
    hidden = (swish * up_pre).astype(jnp.bfloat16)
    hidden_cot = jnp.dot(cot_block, down_w.T, preferred_element_type=jnp.float32)
    grad_down = jnp.dot(hidden.T, cot_block, preferred_element_type=jnp.float32)
    gate_cot = (hidden_cot * up_pre * sigma * (1.0 + gate_pre * (1.0 - sigma))).astype(jnp.bfloat16)
    up_cot = (hidden_cot * swish).astype(jnp.bfloat16)
    grad_gate = jnp.dot(row_block.T, gate_cot, preferred_element_type=jnp.float32)
    grad_up = jnp.dot(row_block.T, up_cot, preferred_element_type=jnp.float32)
    part_width = FF // N_TP
    gate_groups = gate_cot.astype(jnp.float32).reshape(EXP_ROWS, N_TP, part_width)
    up_groups = up_cot.astype(jnp.float32).reshape(EXP_ROWS, N_TP, part_width)
    gate_wide = gate_w.astype(jnp.float32).reshape(D, N_TP, part_width)
    up_wide = up_w.astype(jnp.float32).reshape(D, N_TP, part_width)
    terms = jnp.einsum('rgf,dgf->grd', gate_groups, gate_wide) + jnp.einsum('rgf,dgf->grd', up_groups, up_wide)
    rounded = lax.optimization_barrier(terms.astype(jnp.bfloat16))
    row_cot = lax.optimization_barrier(jnp.sum(rounded.astype(jnp.float32), axis=0)).astype(jnp.bfloat16)
    return (grad_gate, grad_up, grad_down, row_cot)

def reference(layer_input, out_cot, expert_ids, route_weight, w_gate, w_up, w_down, out_proj, rec_input, gate_input, prev_state, decay_param, extra_decay, gate_a_w, gate_i_w):
    slot_total = TOKENS * TOP
    device_ids = expert_ids.reshape(N_SP, TOK_DEV * TOP)
    onehot = (device_ids[:, :, None] == jnp.arange(EXPERTS, dtype=jnp.int32)[None, None, :]).astype(jnp.int32)
    earlier_count = lax.optimization_barrier(jnp.sum((jnp.cumsum(onehot, axis=1) - onehot) * onehot, axis=2)).astype(jnp.int32)
    source_index = jnp.arange(N_SP, dtype=jnp.int32)[:, None]
    places = (source_index * CAP + earlier_count).reshape(slot_total).astype(jnp.int32)
    flat_ids = expert_ids.reshape(slot_total).astype(jnp.int32)
    token_index = jnp.arange(slot_total, dtype=jnp.int32) // TOP
    weighted = (route_weight[:, :, None] * out_cot[:, None, :].astype(jnp.float32)).astype(jnp.bfloat16).reshape(slot_total, D)
    row_buffer = jnp.zeros((EXPERTS, EXP_ROWS, D), jnp.bfloat16).at[flat_ids, places].set(layer_input[token_index])
    cot_buffer = jnp.zeros((EXPERTS, EXP_ROWS, D), jnp.bfloat16).at[flat_ids, places].set(weighted)
    grad_gate, grad_up, grad_down, back_buffer = lax.map(expert_backward, (row_buffer, cot_buffer, w_gate, w_up, w_down))
    slot_cot = back_buffer[flat_ids, places].astype(jnp.float32).reshape(TOKENS, TOP, D)
    layer_cot = (out_cot.astype(jnp.float32) + lax.optimization_barrier(jnp.sum(slot_cot, axis=1))).astype(jnp.bfloat16)
    mix_cot = jnp.dot(layer_cot, out_proj, preferred_element_type=jnp.float32)
    rgate = jax.nn.sigmoid(head_product(rec_input, gate_a_w, False))
    igate = jax.nn.sigmoid(head_product(rec_input, gate_i_w, False))
    rate_scale = decay_factor * jax.nn.softplus(-decay_param)
    log_decay = -rate_scale[None, :] * rgate + jnp.repeat(extra_decay.T, HEAD_DIM, axis=1)
    decay = jnp.exp(log_decay)
    scale = jnp.sqrt(-jnp.expm1(2.0 * log_decay))
    values_in = rec_input.astype(jnp.float32)
    state = decay * prev_state + scale * igate * values_in
    gate_act, gate_slope = gelu_pair(gate_input.astype(jnp.float32))
    rec_output = (state * gate_act).astype(jnp.bfloat16)
    grad_out_proj = jnp.dot(layer_cot.T, rec_output, preferred_element_type=jnp.float32)
    next_decay = jnp.concatenate([decay[1:], jnp.zeros((1, D_LRU), jnp.float32)], axis=0)
    drive = mix_cot * gate_act
    _, state_cot = lax.associative_scan(chain_link, (next_decay, drive), reverse=True)
    gate_input_grad = (mix_cot * state * gate_slope).astype(jnp.bfloat16)
    log_cot = state_cot * (decay * prev_state - decay * decay / scale * igate * values_in)
    a_pre_cot = (log_cot * -rate_scale[None, :] * rgate * (1.0 - rgate)).astype(jnp.bfloat16)
    i_pre_cot = (state_cot * scale * values_in * igate * (1.0 - igate)).astype(jnp.bfloat16)
    rec_input_grad = (state_cot * scale * igate + head_product(a_pre_cot, gate_a_w, True) + head_product(i_pre_cot, gate_i_w, True)).astype(jnp.bfloat16)
    return (grad_gate, grad_up, grad_down, grad_out_proj, rec_input_grad, gate_input_grad)
```

```python
import functools

import jax
import jax.numpy as jnp
from jax import lax
from jax.experimental import pallas as pl
from jax.experimental.pallas import tpu as pltpu
from jax.sharding import PartitionSpec as P

gelu_scale = 0.7978845608028654
gelu_cubic = 0.044715
decay_factor = 8.0


def exchange_kernel(kinds, axis, *refs):
    pairs = len(kinds)
    sources, targets = refs[:pairs], refs[pairs : 2 * pairs]
    send_sem, recv_sem, local_sem = refs[2 * pairs :]
    count = targets[0].shape[0]
    place = lax.axis_index(axis)
    barrier = pltpu.get_barrier_semaphore()
    for step in range(1, count):
        pl.semaphore_signal(
            barrier,
            inc=1,
            device_id={axis: lax.rem(place + step, count)},
            device_id_type=pl.DeviceIdType.MESH,
        )
    pl.semaphore_wait(barrier, count - 1)
    copies = []
    for which in range(pairs):
        for step in range(1, count):
            peer = lax.rem(place + step, count)
            source = sources[which].at[peer] if kinds[which] else sources[which]
            copy = pltpu.make_async_remote_copy(
                src_ref=source,
                dst_ref=targets[which].at[place],
                send_sem=send_sem.at[which, step],
                recv_sem=recv_sem.at[which, step],
                device_id={axis: peer},
                device_id_type=pl.DeviceIdType.MESH,
            )
            copy.start()
            copies.append(copy)
    for which in range(pairs):
        source = sources[which].at[place] if kinds[which] else sources[which]
        copy = pltpu.make_async_copy(source, targets[which].at[place], local_sem.at[which])
        copy.start()
        copies.append(copy)
    for copy in copies:
        copy.wait()


def exchange(arrays, kinds, axis, number):
    count = lax.axis_size(axis)
    shapes = [
        jax.ShapeDtypeStruct(a.shape if kind else (count,) + a.shape, a.dtype)
        for a, kind in zip(arrays, kinds)
    ]
    spec = pl.BlockSpec(memory_space=pltpu.VMEM)
    return pl.pallas_call(
        functools.partial(exchange_kernel, kinds, axis),
        in_specs=[spec] * len(arrays),
        out_specs=[spec] * len(arrays),
        out_shape=shapes,
        scratch_shapes=[
            pltpu.SemaphoreType.DMA((len(arrays), count)),
            pltpu.SemaphoreType.DMA((len(arrays), count)),
            pltpu.SemaphoreType.DMA((len(arrays),)),
        ],
        compiler_params=pltpu.CompilerParams(collective_id=number, has_side_effects=True),
        cost_estimate=pl.CostEstimate(
            flops=0, bytes_accessed=40 * arrays[0].size, transcendentals=0
        ),
    )(*arrays)


def flipped(index, mask, count):
    result = index
    bit = 1
    while bit < count:
        own = (index // bit) % 2
        turn = (mask // bit) % 2
        result = result + bit * turn * (1 - 2 * own)
        bit *= 2
    return result


def columns_dot(left, right):
    return lax.dot_general(left, right, (((1,), (1,)), ((), ())), preferred_element_type=jnp.float32)


def rows_dot(left, right):
    return lax.dot_general(left, right, (((0,), (0,)), ((), ())), preferred_element_type=jnp.float32)


def expert_kernel(
    rows_out,
    cot_out,
    w_gate_in,
    w_up_in,
    w_down_in,
    returned,
    gate_grad_out,
    up_grad_out,
    down_grad_out,
    x_buf,
    c_buf,
    part_buf,
    near_buf,
    far_send,
    kept,
    far_buf,
    back_send,
    gate_c,
    up_c,
    hidden_buf,
    w_gate,
    w_up,
    w_down,
    gate_grad,
    up_grad,
    down_grad,
    z_sems,
    x_sems,
    d_sems,
    near_sems,
    far_sems,
    back_sems,
    load_sems,
    store_sems,
):
    count, pieces, cap, piece = x_buf.shape
    place = lax.axis_index("sp")
    me = lax.axis_index("tp")
    half = pieces // 2
    far = lax.rem(me + half, pieces)
    near = flipped(me, 1, 2)
    cross = lax.rem(near + half, pieces)
    mesh_ids = pl.DeviceIdType.MESH
    loads = [
        pltpu.make_async_copy(hbm, vmem, load_sems.at[i])
        for i, (hbm, vmem) in enumerate(
            [(w_gate_in, w_gate), (w_up_in, w_up), (w_down_in, w_down)]
        )
    ]
    for load in loads:
        load.start()

    barrier = pltpu.get_barrier_semaphore()

    def greet(step, carry):
        pl.semaphore_signal(
            barrier, inc=1, device_id={"sp": flipped(place, step, count)}, device_id_type=mesh_ids
        )
        return carry

    lax.fori_loop(1, count, greet, 0)
    for other in (far, near):
        pl.semaphore_signal(barrier, inc=1, device_id={"tp": other}, device_id_type=mesh_ids)
    pl.semaphore_wait(barrier, count + 1)

    bufs = (x_buf, c_buf)
    outs = (rows_out, cot_out)

    def remote(source, target, sems, index, axis, other):
        return pltpu.make_async_remote_copy(
            src_ref=source,
            dst_ref=target,
            send_sem=sems.at[(0,) + index],
            recv_sem=sems.at[(1,) + index],
            device_id={axis: other},
            device_id_type=mesh_ids,
        )

    def z_copy(which, step):
        other = flipped(place, step, count)
        return remote(
            outs[which].at[other], bufs[which].at[place, me], z_sems, (which, step), "sp", other
        )

    def x_copy(which, step, source=None):
        ref = bufs[which].at[flipped(place, step, count), me]
        return remote(ref if source is None else source, ref, x_sems, (which, step), "tp", far)

    def d_copy(which, turn, step, source=None):
        ref = bufs[which].at[flipped(place, step, count), far if turn else me]
        return remote(
            ref if source is None else source, ref, d_sems, (which, turn, step), "tp", near
        )

    def near_copy(turn, step):
        origin = flipped(place, step, count)
        return remote(
            part_buf.at[origin, cross if turn else near],
            near_buf.at[origin, turn],
            near_sems,
            (turn, step),
            "tp",
            near,
        )

    def far_copy(step):
        origin = flipped(place, step, count)
        return remote(far_send.at[origin], far_buf.at[origin], far_sems, (step,), "tp", far)

    def back_copy(step):
        origin = flipped(place, step, count)
        return remote(
            back_send.at[origin], returned.at[place], back_sems, (step,), "sp", origin
        )

    def send_all(step, carry):
        for which in range(2):
            z_copy(which, step).start()
        return carry

    lax.fori_loop(1, count, send_all, 0)
    for which in range(2):
        x_copy(which, 0, outs[which].at[place]).start()
        d_copy(which, 0, 0, outs[which].at[place]).start()
    for which in range(2):
        bufs[which][place, me] = outs[which][place]
    for load in loads:
        load.wait()

    def arrive(step):
        for which in range(2):
            z_copy(which, step).wait_recv()
            x_copy(which, step).start()
            d_copy(which, 0, step).start()

    def pass_on(step):
        for which in range(2):
            x_copy(which, step).wait_recv()
            d_copy(which, 1, step).start()

    def compute(step):
        origin = flipped(place, step, count)
        for which in range(2):
            for turn in range(2):
                d_copy(which, turn, step).wait_recv()
        width = w_gate.shape[2]
        gate_pre = jnp.zeros((cap, width), jnp.float32)
        up_pre = jnp.zeros((cap, width), jnp.float32)
        hidden_cot = jnp.zeros((cap, width), jnp.float32)
        for p in range(pieces):
            row_block = x_buf[origin, p]
            gate_pre += jnp.dot(row_block, w_gate[p], preferred_element_type=jnp.float32)
            up_pre += jnp.dot(row_block, w_up[p], preferred_element_type=jnp.float32)
            hidden_cot += columns_dot(c_buf[origin, p], w_down[:, p * piece : (p + 1) * piece])
        sigma = jax.nn.sigmoid(gate_pre)
        swish = gate_pre * sigma
        hidden_buf[origin] = (swish * up_pre).astype(jnp.bfloat16)
        gate_cot = (hidden_cot * up_pre * sigma * (1.0 + gate_pre * (1.0 - sigma))).astype(
            jnp.bfloat16
        )
        up_cot = (hidden_cot * swish).astype(jnp.bfloat16)
        gate_c[origin] = gate_cot
        up_c[origin] = up_cot
        for p in range(pieces):
            part_buf[origin, p] = (
                columns_dot(gate_cot, w_gate[p]) + columns_dot(up_cot, w_up[p])
            ).astype(jnp.bfloat16)
        for turn in range(2):
            near_copy(turn, step).start()

    def halve(step):
        origin = flipped(place, step, count)
        for turn in range(2):
            near_copy(turn, step).wait_recv()
        far_send[origin] = (
            part_buf[origin, far].astype(jnp.float32) + near_buf[origin, 1].astype(jnp.float32)
        ).astype(jnp.bfloat16)
        far_copy(step).start()
        kept[origin] = part_buf[origin, me].astype(jnp.float32) + near_buf[origin, 0].astype(
            jnp.float32
        )

    def finish(step):
        origin = flipped(place, step, count)
        far_copy(step).wait_recv()
        total = (kept[origin] + far_buf[origin].astype(jnp.float32)).astype(jnp.bfloat16)

        @pl.when(step == 0)
        def _():
            returned[place] = total

        @pl.when(step > 0)
        def _():
            back_send[origin] = total
            back_copy(step).start()

    def stage(action, step, first):
        @pl.when((step >= first) & (step < count))
        def _():
            action(step)

    def run(step, carry):
        stage(arrive, step, 1)
        stage(pass_on, step - 1, 0)
        stage(halve, step - 2, 0)
        stage(finish, step - 3, 0)
        stage(compute, step - 1, 0)
        return carry

    lax.fori_loop(0, count + 3, run, 0)

    width = w_gate.shape[2]
    tile = min(piece, 256)
    rows = count * cap
    flat = cap % 16 == 0

    def over_rows(left, right):
        if flat:
            return rows_dot(left().reshape(rows, -1), right().reshape(rows, -1))
        total = rows_dot(left()[0], right()[0])
        for s in range(1, count):
            total = total + rows_dot(left()[s], right()[s])
        return total

    def gradients(p, carry):
        for t in range(piece // tile):
            spot = pl.ds(pl.multiple_of(p * piece + t * tile, tile), tile)
            cut = slice(t * tile, (t + 1) * tile)
            gate_grad[spot, :] = over_rows(lambda: x_buf[:, p, :, cut], lambda: gate_c[...])
            up_grad[spot, :] = over_rows(lambda: x_buf[:, p, :, cut], lambda: up_c[...])
            down_grad[:, spot] = over_rows(lambda: hidden_buf[...], lambda: c_buf[:, p, :, cut])
        return carry

    lax.fori_loop(0, pieces, gradients, 0)
    stores = [
        pltpu.make_async_copy(vmem, hbm, store_sems.at[i])
        for i, (vmem, hbm) in enumerate(
            [
                (gate_grad, gate_grad_out),
                (up_grad, up_grad_out),
                (down_grad, down_grad_out),
            ]
        )
    ]
    for store in stores:
        store.start()

    def settle(step, carry):
        for which in range(2):
            x_copy(which, step).wait_send()
            for turn in range(2):
                d_copy(which, turn, step).wait_send()
        for turn in range(2):
            near_copy(turn, step).wait_send()
        far_copy(step).wait_send()
        return carry

    def settle_far(step, carry):
        for which in range(2):
            z_copy(which, step).wait_send()
        back_copy(step).wait()
        return carry

    lax.fori_loop(0, count, settle, 0)
    lax.fori_loop(1, count, settle_far, 0)
    for store in stores:
        store.wait()


def expert_pass(rows_out, cot_out, w_gate, w_up, w_down, number):
    count, cap, piece = rows_out.shape
    width, hidden_width = w_gate.shape
    pieces = width // piece
    dtype = rows_out.dtype
    f32 = jnp.float32
    vmem = pl.BlockSpec(memory_space=pltpu.VMEM)
    anywhere = pl.BlockSpec(memory_space=pl.ANY)

    def sems(*dims):
        return pltpu.SemaphoreType.DMA(dims)

    return pl.pallas_call(
        expert_kernel,
        in_specs=[vmem, vmem, anywhere, anywhere, anywhere],
        out_specs=[vmem, anywhere, anywhere, anywhere],
        out_shape=[
            jax.ShapeDtypeStruct((count, cap, piece), dtype),
            jax.ShapeDtypeStruct((width, hidden_width), f32),
            jax.ShapeDtypeStruct((width, hidden_width), f32),
            jax.ShapeDtypeStruct((hidden_width, width), f32),
        ],
        scratch_shapes=[
            pltpu.VMEM((count, pieces, cap, piece), dtype),
            pltpu.VMEM((count, pieces, cap, piece), dtype),
            pltpu.VMEM((count, pieces, cap, piece), dtype),
            pltpu.VMEM((count, 2, cap, piece), dtype),
            pltpu.VMEM((count, cap, piece), dtype),
            pltpu.VMEM((count, cap, piece), f32),
            pltpu.VMEM((count, cap, piece), dtype),
            pltpu.VMEM((count, cap, piece), dtype),
            pltpu.VMEM((count, cap, hidden_width), dtype),
            pltpu.VMEM((count, cap, hidden_width), dtype),
            pltpu.VMEM((count, cap, hidden_width), dtype),
            pltpu.VMEM((pieces, piece, hidden_width), dtype),
            pltpu.VMEM((pieces, piece, hidden_width), dtype),
            pltpu.VMEM((hidden_width, width), dtype),
            pltpu.VMEM((width, hidden_width), f32),
            pltpu.VMEM((width, hidden_width), f32),
            pltpu.VMEM((hidden_width, width), f32),
            sems(2, 2, count),
            sems(2, 2, count),
            sems(2, 2, 2, count),
            sems(2, 2, count),
            sems(2, count),
            sems(2, count),
            sems(3),
            sems(3),
        ],
        compiler_params=pltpu.CompilerParams(
            collective_id=number, has_side_effects=True, vmem_limit_bytes=60 * 1024 * 1024
        ),
        cost_estimate=pl.CostEstimate(
            flops=18 * count * cap * width * hidden_width,
            bytes_accessed=40 * rows_out.size,
            transcendentals=0,
        ),
    )(
        rows_out,
        cot_out,
        w_gate.reshape(pieces, piece, hidden_width),
        w_up.reshape(pieces, piece, hidden_width),
        w_down,
    )


def carried_in(gathered, axis):
    count = lax.axis_size(axis)
    place = lax.axis_index(axis)
    carry = jnp.zeros_like(gathered[0, 0])
    for source in range(count - 1, 0, -1):
        step = gathered[source, 1] + gathered[source, 0] * carry
        carry = jnp.where(source > place, step, carry)
    return carry


def scan_kernel(link_ref, drive_ref, product_ref, total_ref):
    link = link_ref[...]
    total = drive_ref[...]
    rows, cols = link.shape
    row_index = lax.broadcasted_iota(jnp.int32, (rows, cols), 0)
    step = 1
    while step < rows:
        if step < 8:
            inside = row_index < rows - step
            later_link = jnp.where(inside, pltpu.roll(link, rows - step, 0), 1.0)
            later_total = jnp.where(inside, pltpu.roll(total, rows - step, 0), 0.0)
        else:
            later_link = jnp.concatenate([link[step:], jnp.ones((step, cols), jnp.float32)], axis=0)
            later_total = jnp.concatenate(
                [total[step:], jnp.zeros((step, cols), jnp.float32)], axis=0
            )
        total = total + link * later_total
        link = link * later_link
        step *= 2
    product_ref[...] = link
    total_ref[...] = total


def reverse_scan(link, drive):
    rows, cols = link.shape
    lanes = 128
    spec = pl.BlockSpec((rows, lanes), lambda i: (0, i))
    return pl.pallas_call(
        scan_kernel,
        grid=(cols // lanes,),
        in_specs=[spec, spec],
        out_specs=[spec, spec],
        out_shape=[jax.ShapeDtypeStruct((rows, cols), jnp.float32)] * 2,
        cost_estimate=pl.CostEstimate(
            flops=40 * rows * cols, bytes_accessed=16 * rows * cols, transcendentals=0
        ),
    )(link, drive)


def gelu_pair(values_in):
    inner = gelu_scale * (values_in + gelu_cubic * values_in * values_in * values_in)
    bend = jnp.tanh(inner)
    active = 0.5 * values_in * (1.0 + bend)
    slope = 0.5 * (1.0 + bend) + 0.5 * values_in * (1.0 - bend * bend) * gelu_scale * (
        1.0 + 3.0 * gelu_cubic * values_in * values_in
    )
    return (active, slope)


def head_product(row_block, weights, backward):
    heads = weights.shape[0]
    head_width = weights.shape[1]
    blocks = row_block.reshape(row_block.shape[0], heads, head_width)
    if backward:
        result = jnp.einsum("nhe,hde->nhd", blocks, weights, preferred_element_type=jnp.float32)
    else:
        result = jnp.einsum("nhd,hde->nhe", blocks, weights, preferred_element_type=jnp.float32)
    return result.reshape(row_block.shape[0], heads * head_width)


def slot_places(expert_ids, expert_count, capacity):
    flat_ids = expert_ids.reshape(-1)
    onehot = (flat_ids[:, None] == jnp.arange(expert_count, dtype=jnp.int32)[None, :]).astype(
        jnp.int32
    )
    earlier_count = jnp.sum((jnp.cumsum(onehot, axis=0) - onehot) * onehot, axis=1)
    return flat_ids * capacity + earlier_count


def per_device(
    layer_input,
    out_cot,
    expert_ids,
    route_weight,
    w_gate,
    w_up,
    w_down,
    out_proj,
    rec_input,
    gate_input,
    prev_state,
    decay_param,
    extra_decay,
    gate_a_w,
    gate_i_w,
):
    sources = lax.axis_size("sp")
    local_experts = w_gate.shape[0]
    expert_count = local_experts * sources
    tok_rows, width = layer_input.shape
    top_count = expert_ids.shape[1]
    capacity = 5 * tok_rows * top_count // (4 * expert_count)
    slot_count = tok_rows * top_count
    places = slot_places(expert_ids, expert_count, capacity)
    buffer_rows = expert_count * capacity
    token_places = places.reshape(tok_rows, top_count)
    row_index = jnp.arange(buffer_rows, dtype=jnp.int32)
    hits = row_index[:, None, None] == token_places.T[None, :, :]
    pick = jnp.any(hits, axis=1).astype(jnp.bfloat16)
    row_weight = jnp.sum(jnp.where(hits, route_weight.T[None, :, :], 0.0), axis=(1, 2))
    members = lax.axis_size("tp")
    piece = width // members
    first_col = lax.rem(lax.axis_index("tp"), members) * piece

    def outgoing_rows(array, weight):
        cols = lax.dynamic_slice_in_dim(array, first_col, piece, 1)
        rows = jnp.dot(pick, cols, preferred_element_type=jnp.float32)
        if weight is not None:
            rows = rows * weight[:, None]
        return rows.astype(jnp.bfloat16).reshape(sources, buffer_rows // sources, piece)

    returned, grad_gate, grad_up, grad_down = expert_pass(
        outgoing_rows(layer_input, None),
        outgoing_rows(out_cot, row_weight),
        w_gate[0],
        w_up[0],
        w_down[0],
        0,
    )
    grad_gate, grad_up, grad_down = grad_gate[None], grad_up[None], grad_down[None]
    returned = returned.reshape(buffer_rows, piece)
    channels = rec_input.shape[1]
    head_width = gate_a_w.shape[1]
    heads_here = channels // head_width
    first_head = lax.axis_index("tp") * heads_here
    decay_map = lax.dynamic_slice_in_dim(gate_a_w, first_head, heads_here, 0)
    input_map = lax.dynamic_slice_in_dim(gate_i_w, first_head, heads_here, 0)
    rates = lax.dynamic_slice_in_dim(decay_param, lax.axis_index("tp") * channels, channels, 0)
    rgate = jax.nn.sigmoid(head_product(rec_input, decay_map, False))
    igate = jax.nn.sigmoid(head_product(rec_input, input_map, False))
    rate_scale = decay_factor * jax.nn.softplus(-rates)
    log_decay = -rate_scale[None, :] * rgate + jnp.repeat(extra_decay.T, head_width, axis=1)
    decay = jnp.exp(log_decay)
    scale = jnp.sqrt(-jnp.expm1(2.0 * log_decay))
    values_in = rec_input.astype(jnp.float32)
    state = decay * prev_state + scale * igate * values_in
    gate_act, _ = gelu_pair(gate_input.astype(jnp.float32))
    rec_output = (state * gate_act).astype(jnp.bfloat16)
    col_count = piece
    slot_sum = lax.dot_general(
        pick, returned, (((0,), (0,)), ((), ())), preferred_element_type=jnp.float32
    )
    own_cot = lax.dynamic_slice_in_dim(out_cot, lax.axis_index("tp") * col_count, col_count, 1)
    part_cot = (own_cot.astype(jnp.float32) + slot_sum).astype(jnp.bfloat16)
    layer_cot = lax.all_gather(part_cot, "tp", axis=1, tiled=True)
    mix_cot = jnp.dot(layer_cot, out_proj, preferred_element_type=jnp.float32)
    decay = jnp.exp(log_decay)
    scale = jnp.sqrt(-jnp.expm1(2.0 * log_decay))
    values_in = rec_input.astype(jnp.float32)
    state = decay * prev_state + scale * igate * values_in
    gate_act, gate_slope = gelu_pair(gate_input.astype(jnp.float32))
    out_term = lax.dot_general(
        layer_cot, rec_output, (((0,), (0,)), ((), ())), preferred_element_type=jnp.float32
    ).astype(jnp.bfloat16)
    link = jnp.concatenate([decay[1:], jnp.ones((1, channels), jnp.float32)], axis=0)
    products, local_cot = reverse_scan(link, mix_cot * gate_act)
    edge = jnp.stack([decay[0] * products[0], decay[0] * local_cot[0]])
    edge = jnp.concatenate([edge, jnp.zeros((6, channels), jnp.float32)], axis=0)
    out_blocks = out_term.reshape(sources, width // sources, channels)
    gathered, out_terms = exchange([edge, out_blocks], [False, True], "sp", 3)
    grad_out_proj = jnp.sum(out_terms.astype(jnp.float32), axis=0)
    carried = carried_in(gathered, "sp")
    state_cot = local_cot + products * carried[None, :]
    gate_input_grad = (mix_cot * state * gate_slope).astype(jnp.bfloat16)
    log_cot = state_cot * (decay * prev_state - decay * decay / scale * igate * values_in)
    a_pre_cot = (log_cot * -rate_scale[None, :] * rgate * (1.0 - rgate)).astype(jnp.bfloat16)
    i_pre_cot = (state_cot * scale * values_in * igate * (1.0 - igate)).astype(jnp.bfloat16)
    rec_input_grad = (
        state_cot * scale * igate
        + head_product(a_pre_cot, decay_map, True)
        + head_product(i_pre_cot, input_map, True)
    ).astype(jnp.bfloat16)
    return (grad_gate, grad_up, grad_down, grad_out_proj, rec_input_grad, gate_input_grad)


def solution(mesh):
    in_specs = (
        P("sp", None),
        P("sp", None),
        P("sp", None),
        P("sp", None),
        P("sp", None, "tp"),
        P("sp", None, "tp"),
        P("sp", "tp", None),
        P(None, "tp"),
        P("sp", "tp"),
        P("sp", "tp"),
        P("sp", "tp"),
        P(),
        P("tp", "sp"),
        P(),
        P(),
    )
    out_specs = (
        P("sp", None, "tp"),
        P("sp", None, "tp"),
        P("sp", "tp", None),
        P("sp", "tp"),
        P("sp", "tp"),
        P("sp", "tp"),
    )
    return jax.shard_map(
        per_device, mesh=mesh, in_specs=in_specs, out_specs=out_specs, check_vma=False
    )
```

```python
import jax
import jax.numpy as jnp
from jax import lax
from jax.experimental import pallas as pl
from jax.experimental.pallas import tpu as pltpu
from jax.sharding import PartitionSpec as P

gelu_scale = 0.7978845608028654
gelu_cubic = 0.044715
decay_factor = 8.0
mesh_ids = pl.DeviceIdType.MESH
f32 = jnp.float32
bf16 = jnp.bfloat16


def flipped(index, mask, count):
    result = index
    bit = 1
    while bit < count:
        own = (index // bit) % 2
        turn = (mask // bit) % 2
        result = result + bit * turn * (1 - 2 * own)
        bit *= 2
    return result


def plain_dot(left, right):
    return jnp.dot(left, right, preferred_element_type=f32)


def columns_dot(left, right):
    return lax.dot_general(left, right, (((1,), (1,)), ((), ())), preferred_element_type=f32)


def rows_dot(left, right):
    return lax.dot_general(left, right, (((0,), (0,)), ((), ())), preferred_element_type=f32)


def gelu_pair(values_in):
    inner = gelu_scale * (values_in + gelu_cubic * values_in * values_in * values_in)
    bend = jnp.tanh(inner)
    active = 0.5 * values_in * (1.0 + bend)
    slope = 0.5 * (1.0 + bend) + 0.5 * values_in * (1.0 - bend * bend) * gelu_scale * (
        1.0 + 3.0 * gelu_cubic * values_in * values_in
    )
    return (active, slope)


def one_minus_exp(value):
    series = value * (
        1.0
        + value * (0.5 + value * (1.0 / 6 + value * (1.0 / 24 + value * (1.0 / 120 + value / 720))))
    )
    return jnp.where(value > -0.25, -series, 1.0 - jnp.exp(value))


def scan_columns(link, total):
    rows, cols = link.shape
    row_index = lax.broadcasted_iota(jnp.int32, (rows, cols), 0)
    step = 1
    while step < rows:
        if step < 8:
            inside = row_index < rows - step
            later_link = jnp.where(inside, pltpu.roll(link, rows - step, 0), 1.0)
            later_total = jnp.where(inside, pltpu.roll(total, rows - step, 0), 0.0)
        else:
            later_link = jnp.concatenate([link[step:], jnp.ones((step, cols), f32)], axis=0)
            later_total = jnp.concatenate([total[step:], jnp.zeros((step, cols), f32)], axis=0)
        total = total + link * later_total
        link = link * later_link
        step *= 2
    return link, total


def step_kernel(*refs):
    (
        layer_in,
        cot_in,
        ids_in,
        route_in,
        w_gate_in,
        w_up_in,
        w_down_in,
        out_proj_in,
        rec_in,
        gate_in,
        prev_in,
        rates_in,
        extra_in,
        map_a_in,
        map_i_in,
        gate_grad_out,
        up_grad_out,
        down_grad_out,
        proj_grad_out,
        rec_grad_out,
        gate_input_out,
        layer_buf,
        cot_buf,
        pick_buf,
        rows_out,
        cot_out,
        x_buf,
        c_buf,
        part_buf,
        near_buf,
        far_send,
        far_buf,
        back_send,
        returned,
        gate_c,
        up_c,
        hidden_buf,
        w_gate,
        w_up,
        w_down,
        out_proj,
        gate_grad,
        up_grad,
        down_grad,
        rgate_buf,
        igate_buf,
        decay_buf,
        scale_buf,
        state_buf,
        act_buf,
        slope_buf,
        rec_out,
        full_cot,
        mix_buf,
        term_send,
        term_buf,
        edge_send,
        edge_buf,
        product_buf,
        local_buf,
        z_sems,
        x_sems,
        d_sems,
        near_sems,
        far_sems,
        back_sems,
        gather_sems,
        term_sems,
        edge_sems,
        load_sems,
        store_sems,
    ) = refs
    count, pieces, cap, piece = x_buf.shape
    tokens, channels = rec_in.shape
    head_width = map_a_in.shape[1]
    heads = channels // head_width
    place = lax.axis_index("sp")
    me = lax.axis_index("tp")
    half = pieces // 2
    far = lax.rem(me + half, pieces)
    near = flipped(me, 1, 2)
    cross = lax.rem(near + half, pieces)
    near_count = count // 2

    loads = []
    for p in range(pieces):
        cut = pl.ds(p * piece, piece)
        loads.append((layer_in.at[:, cut], layer_buf.at[p]))
        loads.append((cot_in.at[:, cut], cot_buf.at[p]))
    early = len(loads)
    loads += [(w_gate_in, w_gate), (w_up_in, w_up), (w_down_in, w_down), (out_proj_in, out_proj)]
    loads = [pltpu.make_async_copy(a, b, load_sems.at[i]) for i, (a, b) in enumerate(loads)]
    for load in loads:
        load.start()

    barrier = pltpu.get_barrier_semaphore()

    def greet(step, carry):
        pl.semaphore_signal(
            barrier, inc=1, device_id={"sp": flipped(place, step, count)}, device_id_type=mesh_ids
        )
        return carry

    lax.fori_loop(1, count, greet, 0)
    for other in (far, near):
        pl.semaphore_signal(barrier, inc=1, device_id={"tp": other}, device_id_type=mesh_ids)

    expert_index = lax.broadcasted_iota(jnp.int32, (count, tokens), 0)
    first = (expert_index == ids_in[0:1, :]).astype(f32)
    second = (expert_index == ids_in[1:2, :]).astype(f32)
    earlier = (
        lax.broadcasted_iota(jnp.int32, (tokens, tokens), 0)
        < lax.broadcasted_iota(jnp.int32, (tokens, tokens), 1)
    ).astype(f32)
    before = plain_dot((first + second).astype(bf16), earlier.astype(bf16))
    spots = before + (cap * expert_index).astype(f32)
    first_place = jnp.sum(first * spots, axis=0, keepdims=True)
    second_place = jnp.sum(second * spots, axis=0, keepdims=True)
    row_index = lax.broadcasted_iota(jnp.int32, (cap, tokens), 0)

    def picks(target):
        rows = (row_index + target * cap).astype(f32)
        hit_first = rows == first_place
        hit_second = rows == second_place
        pick = jnp.where(hit_first | hit_second, 1.0, 0.0).astype(bf16)
        weight = jnp.sum(
            jnp.where(hit_first, route_in[0:1, :], 0.0)
            + jnp.where(hit_second, route_in[1:2, :], 0.0),
            axis=1,
            keepdims=True,
        )
        pick_buf[target] = pick
        return pick, weight

    bufs = (x_buf, c_buf)
    outs = (rows_out, cot_out)

    def remote(source, target, sems, index, axis, other):
        return pltpu.make_async_remote_copy(
            src_ref=source,
            dst_ref=target,
            send_sem=sems.at[(0,) + index],
            recv_sem=sems.at[(1,) + index],
            device_id={axis: other},
            device_id_type=mesh_ids,
        )

    def z_copy(which, step):
        other = flipped(place, step, count)
        return remote(
            outs[which].at[other], bufs[which].at[place, me], z_sems, (which, step), "sp", other
        )

    def x_copy(which, step):
        ref = bufs[which].at[flipped(place, step, count), me]
        return remote(ref, ref, x_sems, (which, step), "tp", far)

    def d_copy(which, turn, step):
        ref = bufs[which].at[flipped(place, step, count), far if turn else me]
        return remote(ref, ref, d_sems, (which, turn, step), "tp", near)

    def near_copy(turn, step):
        origin = flipped(place, step, count)
        return remote(
            part_buf.at[origin, cross if turn else near],
            near_buf.at[origin, turn],
            near_sems,
            (turn, step),
            "tp",
            near,
        )

    def far_copy(step):
        origin = flipped(place, step, count)
        return remote(far_send.at[origin], far_buf.at[origin], far_sems, (step,), "tp", far)

    def back_copy(step):
        origin = flipped(place, step, count)
        return remote(back_send.at[origin], returned.at[place], back_sems, (step,), "sp", origin)

    def edge_copy(step):
        other = flipped(place, step, count)
        return remote(edge_send, edge_buf.at[place], edge_sems, (step,), "sp", other)

    def gather_copy(turn):
        if turn == 0:
            return remote(full_cot.at[me], full_cot.at[me], gather_sems, (0,), "tp", far)
        ref = full_cot.at[me if turn == 1 else far]
        return remote(ref, ref, gather_sems, (turn,), "tp", near)

    for load in loads[:early]:
        load.wait()
    pl.semaphore_wait(barrier, count + 1)

    def send_rows(step, carry):
        target = flipped(place, step, count)
        pick, weight = picks(target)
        rows_out[target] = plain_dot(pick, layer_buf[me]).astype(bf16)
        z_copy(0, step).start()
        cot_out[target] = (plain_dot(pick, cot_buf[me]) * weight).astype(bf16)
        z_copy(1, step).start()
        return carry

    lax.fori_loop(1, count, send_rows, 0)
    pick, weight = picks(place)
    for p in range(pieces):
        x_buf[place, p] = plain_dot(pick, layer_buf[p]).astype(bf16)
        c_buf[place, p] = (plain_dot(pick, cot_buf[p]) * weight).astype(bf16)
    for load in loads[early:]:
        load.wait()

    def recurrence():
        rate = rates_in[me]
        rate_scale = decay_factor * (
            jnp.maximum(-rate, 0.0) + jnp.log1p(jnp.exp(-jnp.abs(rate)))
        )
        extra = extra_in[...]
        if heads % 8:
            extra = jnp.concatenate([extra, jnp.zeros((8 - heads % 8, tokens), f32)], axis=0)
        extra = extra.T
        for h in range(heads):
            cut = slice(h * head_width, (h + 1) * head_width)
            rows = rec_in[:, cut]
            rgate = jax.nn.sigmoid(plain_dot(rows, map_a_in[me * heads + h]))
            igate = jax.nn.sigmoid(plain_dot(rows, map_i_in[me * heads + h]))
            log_decay = -rate_scale[:, cut] * rgate + extra[:, h : h + 1]
            decay = jnp.exp(log_decay)
            scale = jnp.sqrt(one_minus_exp(2.0 * log_decay))
            state = decay * prev_in[:, cut] + scale * igate * rows.astype(f32)
            act, slope = gelu_pair(gate_in[:, cut].astype(f32))
            rgate_buf[:, cut] = rgate
            igate_buf[:, cut] = igate
            decay_buf[:, cut] = decay
            scale_buf[:, cut] = scale
            state_buf[:, cut] = state
            act_buf[:, cut] = act
            slope_buf[:, cut] = slope
            rec_out[:, cut] = (state * act).astype(bf16)
        return rate_scale

    rate_scale = recurrence()

    def arrive(step):
        for which in range(2):
            z_copy(which, step).wait_recv()
            x_copy(which, step).start()
            d_copy(which, 0, step).start()

    def pass_on(step):
        for which in range(2):
            x_copy(which, step).wait_recv()
            d_copy(which, 1, step).start()
        for which in range(2):
            for turn in range(2):
                d_copy(which, turn, step).wait_recv()

    def compute(step):
        origin = flipped(place, step, count)
        width = w_gate.shape[2]
        gate_pre = jnp.zeros((cap, width), f32)
        up_pre = jnp.zeros((cap, width), f32)
        hidden_cot = jnp.zeros((cap, width), f32)
        for p in range(pieces):
            row_block = x_buf[origin, p]
            gate_pre += plain_dot(row_block, w_gate[p])
            up_pre += plain_dot(row_block, w_up[p])
            hidden_cot += columns_dot(c_buf[origin, p], w_down[:, p * piece : (p + 1) * piece])
        sigma = jax.nn.sigmoid(gate_pre)
        swish = gate_pre * sigma
        hidden_buf[origin] = (swish * up_pre).astype(bf16)
        gate_cot = (hidden_cot * up_pre * sigma * (1.0 + gate_pre * (1.0 - sigma))).astype(bf16)
        up_cot = (hidden_cot * swish).astype(bf16)
        gate_c[origin] = gate_cot
        up_c[origin] = up_cot
        for p in range(pieces):
            part_buf[origin, p] = (
                columns_dot(gate_cot, w_gate[p]) + columns_dot(up_cot, w_up[p])
            ).astype(bf16)
        for turn in range(2):
            near_copy(turn, step).start()

    def halve(step):
        origin = flipped(place, step, count)
        for turn in range(2):
            near_copy(turn, step).wait_recv()
        far_send[origin] = (
            part_buf[origin, far].astype(f32) + near_buf[origin, 1].astype(f32)
        ).astype(bf16)
        far_copy(step).start()

    def finish(step):
        origin = flipped(place, step, count)
        far_copy(step).wait_recv()
        total = (
            part_buf[origin, me].astype(f32)
            + near_buf[origin, 0].astype(f32)
            + far_buf[origin].astype(f32)
        ).astype(bf16)

        @pl.when(step == 0)
        def _():
            returned[place] = total

        @pl.when(step > 0)
        def _():
            back_send[origin] = total
            back_copy(step).start()

    def run(step, carry):
        @pl.when(step + 1 < near_count)
        def _():
            arrive(step + 1)

        @pl.when(step >= near_count)
        def _():
            arrive(step)

        @pl.when(step >= 1)
        def _():
            finish(step - 1)
            pass_on(step)

        compute(step)
        halve(step)
        return carry

    lax.fori_loop(0, count, run, 0)

    width = w_gate.shape[2]
    tile = min(piece, 256)
    rows = count * cap

    def over_rows(left, right):
        if cap % 16 == 0:
            return rows_dot(left().reshape(rows, -1), right().reshape(rows, -1))
        total = rows_dot(left()[0], right()[0])
        for s in range(1, count):
            total = total + rows_dot(left()[s], right()[s])
        return total

    def gradients(p, carry):
        for t in range(piece // tile):
            spot = pl.ds(pl.multiple_of(p * piece + t * tile, tile), tile)
            cut = slice(t * tile, (t + 1) * tile)
            gate_grad[spot, :] = over_rows(lambda: x_buf[:, p, :, cut], lambda: gate_c[...])
            up_grad[spot, :] = over_rows(lambda: x_buf[:, p, :, cut], lambda: up_c[...])
            down_grad[:, spot] = over_rows(lambda: hidden_buf[...], lambda: c_buf[:, p, :, cut])
        return carry

    lax.fori_loop(0, half, gradients, 0)
    finish(count - 1)
    lax.fori_loop(half, pieces, gradients, 0)
    stores = [
        pltpu.make_async_copy(vmem, hbm, store_sems.at[i])
        for i, (vmem, hbm) in enumerate(
            [
                (gate_grad, gate_grad_out),
                (up_grad, up_grad_out),
                (down_grad, down_grad_out),
            ]
        )
    ]
    for store in stores:
        store.start()

    def add_slots(step, total):
        origin = flipped(place, step, count)
        back_copy(step).wait_recv()
        return total + rows_dot(pick_buf[origin], returned[origin])

    slots = rows_dot(pick_buf[place], returned[place])
    slots = lax.fori_loop(1, count, add_slots, slots)
    full_cot[me] = (cot_buf[me].astype(f32) + slots).astype(bf16)
    gather_copy(0).start()
    gather_copy(1).start()

    term_rows = piece * pieces // count
    per_piece = piece // term_rows

    def term_copy(block):
        return pltpu.make_async_remote_copy(
            src_ref=term_send.at[block],
            dst_ref=term_buf.at[place],
            send_sem=term_sems.at[0, block],
            recv_sem=term_sems.at[1, place],
            device_id={"sp": block},
            device_id_type=mesh_ids,
        )

    def arrival(source):
        return pltpu.make_async_remote_copy(
            src_ref=term_send.at[source],
            dst_ref=term_buf.at[source],
            send_sem=term_sems.at[0, source],
            recv_sem=term_sems.at[1, source],
            device_id={"sp": source},
            device_id_type=mesh_ids,
        )

    def use(p, start):
        block = full_cot[p]
        product = plain_dot(block, out_proj[p])
        if start:
            mix_buf[...] = product
        else:
            mix_buf[...] += product
        for j in range(per_piece):
            target = p * per_piece + j
            cut = slice(j * term_rows, (j + 1) * term_rows)
            term = rows_dot(full_cot[p, :, cut], rec_out[...]).astype(bf16) if (
                term_rows % 128 == 0
            ) else rows_dot(block, rec_out[...])[cut].astype(bf16)
            term_send[target] = term

            @pl.when(target != place)
            def _():
                term_copy(target).start()

            @pl.when(target == place)
            def _():
                term_buf[place] = term

    use(me, True)
    gather_copy(1).wait_recv()
    use(near, False)
    gather_copy(0).wait_recv()
    gather_copy(2).start()
    use(far, False)
    gather_copy(2).wait_recv()
    use(cross, False)

    for h in range(heads):
        cut = slice(h * head_width, (h + 1) * head_width)
        decay = decay_buf[:, cut]
        index = lax.broadcasted_iota(jnp.int32, decay.shape, 0)
        link = jnp.where(index < tokens - 1, pltpu.roll(decay, tokens - 1, 0), 1.0)
        product, total = scan_columns(link, mix_buf[:, cut] * act_buf[:, cut])
        product_buf[:, cut] = product
        local_buf[:, cut] = total
        edge_send[0:1, cut] = decay[0:1] * product[0:1]
        edge_send[1:2, cut] = decay[0:1] * total[0:1]
        edge_send[2:8, cut] = jnp.zeros((6, head_width), f32)

    def send_edge(step, carry):
        edge_copy(step).start()
        return carry

    lax.fori_loop(1, count, send_edge, 0)
    gate_input_out[...] = (mix_buf[...] * state_buf[...] * slope_buf[...]).astype(bf16)

    def wait_edge(step, carry):
        edge_copy(step).wait_recv()
        return carry

    lax.fori_loop(1, count, wait_edge, 0)
    edge_buf[place] = edge_send[...]

    def carry_on(turn, carry):
        source = count - 1 - turn
        step = edge_buf[source, 1:2] + edge_buf[source, 0:1] * carry
        return jnp.where(source > place, step, carry)

    carried = lax.fori_loop(0, count - 1, carry_on, jnp.zeros((1, channels), f32))
    for h in range(heads):
        cut = slice(h * head_width, (h + 1) * head_width)
        values_in = rec_in[:, cut].astype(f32)
        decay, scale = decay_buf[:, cut], scale_buf[:, cut]
        rgate, igate = rgate_buf[:, cut], igate_buf[:, cut]
        state_cot = local_buf[:, cut] + product_buf[:, cut] * carried[:, cut]
        log_cot = state_cot * (
            decay * prev_in[:, cut] - decay * decay / scale * igate * values_in
        )
        a_pre = (log_cot * -rate_scale[:, cut] * rgate * (1.0 - rgate)).astype(bf16)
        i_pre = (state_cot * scale * values_in * igate * (1.0 - igate)).astype(bf16)
        rec_grad_out[:, cut] = (
            state_cot * scale * igate
            + columns_dot(a_pre, map_a_in[me * heads + h])
            + columns_dot(i_pre, map_i_in[me * heads + h])
        ).astype(bf16)

    def wait_term(step, carry):
        arrival(flipped(place, step, count)).wait_recv()
        return carry

    lax.fori_loop(1, count, wait_term, 0)

    def sum_terms(source, total):
        return total + term_buf[source].astype(f32)

    proj_grad_out[...] = lax.fori_loop(
        1, count, sum_terms, term_buf[0].astype(f32)
    )

    def settle(step, carry):
        for turn in range(2):
            near_copy(turn, step).wait_send()
        far_copy(step).wait_send()
        return carry

    def settle_far(step, carry):
        for which in range(2):
            z_copy(which, step).wait_send()
            x_copy(which, step).wait_send()
            for turn in range(2):
                d_copy(which, turn, step).wait_send()
        back_copy(step).wait_send()
        edge_copy(step).wait_send()
        arrival(flipped(place, step, count)).wait_send()
        return carry

    lax.fori_loop(0, count, settle, 0)
    lax.fori_loop(1, count, settle_far, 0)
    for turn in range(3):
        gather_copy(turn).wait_send()
    for store in stores:
        store.wait()


def per_device(
    layer_input,
    out_cot,
    expert_ids,
    route_weight,
    w_gate,
    w_up,
    w_down,
    out_proj,
    rec_input,
    gate_input,
    prev_state,
    decay_param,
    extra_decay,
    gate_a_w,
    gate_i_w,
):
    count = lax.axis_size("sp")
    pieces = lax.axis_size("tp")
    local_experts, width, hidden_width = w_gate.shape
    tokens, channels = rec_input.shape
    top_count = expert_ids.shape[1]
    assert local_experts == 1 and top_count == 2 and pieces == 4
    cap = 5 * tokens * top_count // (4 * count)
    piece = width // pieces
    term_rows = width // count
    head_count, head_width = gate_a_w.shape[:2]
    vmem = pl.BlockSpec(memory_space=pltpu.VMEM)
    anywhere = pl.BlockSpec(memory_space=pl.ANY)

    def sems(*dims):
        return pltpu.SemaphoreType.DMA(dims)

    def buf(*dims, dtype=bf16):
        return pltpu.VMEM(dims, dtype)

    rec_bufs = [buf(tokens, channels, dtype=f32)] * 7
    grads = pl.pallas_call(
        step_kernel,
        in_specs=[
            anywhere,
            anywhere,
            vmem,
            vmem,
            anywhere,
            anywhere,
            anywhere,
            anywhere,
            vmem,
            vmem,
            vmem,
            vmem,
            vmem,
            vmem,
            vmem,
        ],
        out_specs=[anywhere, anywhere, anywhere, vmem, vmem, vmem],
        out_shape=[
            jax.ShapeDtypeStruct((width, hidden_width), f32),
            jax.ShapeDtypeStruct((width, hidden_width), f32),
            jax.ShapeDtypeStruct((hidden_width, width), f32),
            jax.ShapeDtypeStruct((term_rows, channels), f32),
            jax.ShapeDtypeStruct((tokens, channels), bf16),
            jax.ShapeDtypeStruct((tokens, channels), bf16),
        ],
        scratch_shapes=[
            buf(pieces, tokens, piece),
            buf(pieces, tokens, piece),
            buf(count, cap, tokens),
            buf(count, cap, piece),
            buf(count, cap, piece),
            buf(count, pieces, cap, piece),
            buf(count, pieces, cap, piece),
            buf(count, pieces, cap, piece),
            buf(count, 2, cap, piece),
            buf(count, cap, piece),
            buf(count, cap, piece),
            buf(count, cap, piece),
            buf(count, cap, piece),
            buf(count, cap, hidden_width),
            buf(count, cap, hidden_width),
            buf(count, cap, hidden_width),
            buf(pieces, piece, hidden_width),
            buf(pieces, piece, hidden_width),
            buf(hidden_width, width),
            buf(pieces, piece, channels),
            buf(width, hidden_width, dtype=f32),
            buf(width, hidden_width, dtype=f32),
            buf(hidden_width, width, dtype=f32),
            *rec_bufs,
            buf(tokens, channels),
            buf(pieces, tokens, piece),
            buf(tokens, channels, dtype=f32),
            buf(count, term_rows, channels),
            buf(count, term_rows, channels),
            buf(8, channels, dtype=f32),
            buf(count, 8, channels, dtype=f32),
            buf(tokens, channels, dtype=f32),
            buf(tokens, channels, dtype=f32),
            sems(2, 2, count),
            sems(2, 2, count),
            sems(2, 2, 2, count),
            sems(2, 2, count),
            sems(2, count),
            sems(2, count),
            sems(2, 3),
            sems(2, count),
            sems(2, count),
            sems(2 * pieces + 4),
            sems(3),
        ],
        compiler_params=pltpu.CompilerParams(
            collective_id=0, has_side_effects=True, vmem_limit_bytes=63 * 1024 * 1024
        ),
        cost_estimate=pl.CostEstimate(
            flops=18 * count * cap * width * hidden_width,
            bytes_accessed=40 * count * cap * piece,
            transcendentals=0,
        ),
    )(
        layer_input,
        out_cot,
        expert_ids.T,
        route_weight.T,
        w_gate.reshape(pieces, piece, hidden_width),
        w_up.reshape(pieces, piece, hidden_width),
        w_down[0],
        out_proj.reshape(pieces, piece, channels),
        rec_input,
        gate_input,
        prev_state,
        decay_param.reshape(pieces, 1, channels),
        extra_decay,
        gate_a_w,
        gate_i_w,
    )
    grad_gate, grad_up, grad_down, grad_out_proj, rec_input_grad, gate_input_grad = grads
    return (
        grad_gate[None],
        grad_up[None],
        grad_down[None],
        grad_out_proj,
        rec_input_grad,
        gate_input_grad,
    )


def solution(mesh):
    in_specs = (
        P("sp", None),
        P("sp", None),
        P("sp", None),
        P("sp", None),
        P("sp", None, "tp"),
        P("sp", None, "tp"),
        P("sp", "tp", None),
        P(None, "tp"),
        P("sp", "tp"),
        P("sp", "tp"),
        P("sp", "tp"),
        P(),
        P("tp", "sp"),
        P(),
        P(),
    )
    out_specs = (
        P("sp", None, "tp"),
        P("sp", None, "tp"),
        P("sp", "tp", None),
        P("sp", "tp"),
        P("sp", "tp"),
        P("sp", "tp"),
    )
    return jax.shard_map(
        per_device, mesh=mesh, in_specs=in_specs, out_specs=out_specs, check_vma=False
    )
```

```python
import jax
import jax.numpy as jnp
from jax import lax
from jax.experimental import pallas as pl
from jax.experimental.pallas import tpu as pltpu
from jax.sharding import PartitionSpec as P

gelu_scale = 0.7978845608028654
gelu_cubic = 0.044715
decay_factor = 8.0
direct_steps = 2
mesh_ids = pl.DeviceIdType.MESH
f32 = jnp.float32
bf16 = jnp.bfloat16


def flipped(index, mask, count):
    result = index
    bit = 1
    while bit < count:
        own = (index // bit) % 2
        turn = (mask // bit) % 2
        result = result + bit * turn * (1 - 2 * own)
        bit *= 2
    return result


def plain_dot(left, right):
    return jnp.dot(left, right, preferred_element_type=f32)


def columns_dot(left, right):
    return lax.dot_general(left, right, (((1,), (1,)), ((), ())), preferred_element_type=f32)


def rows_dot(left, right):
    return lax.dot_general(left, right, (((0,), (0,)), ((), ())), preferred_element_type=f32)


def gelu_pair(values_in):
    inner = gelu_scale * (values_in + gelu_cubic * values_in * values_in * values_in)
    bend = jnp.tanh(inner)
    active = 0.5 * values_in * (1.0 + bend)
    slope = 0.5 * (1.0 + bend) + 0.5 * values_in * (1.0 - bend * bend) * gelu_scale * (
        1.0 + 3.0 * gelu_cubic * values_in * values_in
    )
    return (active, slope)


def one_minus_exp(value):
    series = value * (
        1.0
        + value * (0.5 + value * (1.0 / 6 + value * (1.0 / 24 + value * (1.0 / 120 + value / 720))))
    )
    return jnp.where(value > -0.25, -series, 1.0 - jnp.exp(value))


def scan_columns(link, total):
    rows, cols = link.shape
    row_index = lax.broadcasted_iota(jnp.int32, (rows, cols), 0)
    step = 1
    while step < rows:
        if step < 8:
            inside = row_index < rows - step
            later_link = jnp.where(inside, pltpu.roll(link, rows - step, 0), 1.0)
            later_total = jnp.where(inside, pltpu.roll(total, rows - step, 0), 0.0)
        else:
            later_link = jnp.concatenate([link[step:], jnp.ones((step, cols), f32)], axis=0)
            later_total = jnp.concatenate([total[step:], jnp.zeros((step, cols), f32)], axis=0)
        total = total + link * later_total
        link = link * later_link
        step *= 2
    return link, total


def step_kernel(*refs):
    (
        layer_in,
        cot_in,
        ids_in,
        route_in,
        w_gate_in,
        w_up_in,
        w_down_in,
        out_proj_in,
        rec_in,
        gate_in,
        prev_in,
        rates_in,
        extra_in,
        map_a_in,
        map_i_in,
        gate_grad_out,
        up_grad_out,
        down_grad_out,
        proj_grad_out,
        rec_grad_out,
        gate_input_out,
        layer_buf,
        cot_buf,
        pick_buf,
        rows_out,
        cot_out,
        rows_more,
        cot_more,
        x_buf,
        c_buf,
        part_buf,
        near_buf,
        far_send,
        far_buf,
        back_send,
        returned,
        gate_c,
        up_c,
        hidden_buf,
        w_gate,
        w_up,
        w_down,
        out_proj,
        gate_grad,
        up_grad,
        down_grad,
        rgate_buf,
        igate_buf,
        decay_buf,
        scale_buf,
        state_buf,
        act_buf,
        slope_buf,
        rec_out,
        full_cot,
        mix_buf,
        term_send,
        term_buf,
        edge_send,
        edge_buf,
        product_buf,
        local_buf,
        z_sems,
        x_sems,
        d_sems,
        near_sems,
        far_sems,
        back_sems,
        gather_sems,
        term_sems,
        edge_sems,
        load_sems,
        store_sems,
    ) = refs
    count, pieces, cap, piece = x_buf.shape
    tokens, channels = rec_in.shape
    head_width = map_a_in.shape[1]
    heads = channels // head_width
    place = lax.axis_index("sp")
    me = lax.axis_index("tp")
    half = pieces // 2
    far = lax.rem(me + half, pieces)
    near = flipped(me, 1, 2)
    cross = lax.rem(near + half, pieces)

    loads = []
    for p in range(pieces):
        cut = pl.ds(p * piece, piece)
        loads.append((layer_in.at[:, cut], layer_buf.at[p]))
        loads.append((cot_in.at[:, cut], cot_buf.at[p]))
    early = len(loads)
    loads += [(w_gate_in, w_gate), (w_up_in, w_up), (w_down_in, w_down), (out_proj_in, out_proj)]
    loads = [pltpu.make_async_copy(a, b, load_sems.at[i]) for i, (a, b) in enumerate(loads)]
    for load in loads:
        load.start()

    barrier = pltpu.get_barrier_semaphore()

    def greet(step, carry):
        pl.semaphore_signal(
            barrier, inc=1, device_id={"sp": flipped(place, step, count)}, device_id_type=mesh_ids
        )
        return carry

    lax.fori_loop(1, count, greet, 0)
    for other in (far, near):
        pl.semaphore_signal(barrier, inc=1, device_id={"tp": other}, device_id_type=mesh_ids)

    expert_index = lax.broadcasted_iota(jnp.int32, (count, tokens), 0)
    first = (expert_index == ids_in[0:1, :]).astype(f32)
    second = (expert_index == ids_in[1:2, :]).astype(f32)
    earlier = (
        lax.broadcasted_iota(jnp.int32, (tokens, tokens), 0)
        < lax.broadcasted_iota(jnp.int32, (tokens, tokens), 1)
    ).astype(f32)
    before = plain_dot((first + second).astype(bf16), earlier.astype(bf16))
    spots = before + (cap * expert_index).astype(f32)
    first_place = jnp.sum(first * spots, axis=0, keepdims=True)
    second_place = jnp.sum(second * spots, axis=0, keepdims=True)
    row_index = lax.broadcasted_iota(jnp.int32, (cap, tokens), 0)

    def picks(target):
        rows = (row_index + target * cap).astype(f32)
        hit_first = rows == first_place
        hit_second = rows == second_place
        pick = jnp.where(hit_first | hit_second, 1.0, 0.0).astype(bf16)
        weight = jnp.sum(
            jnp.where(hit_first, route_in[0:1, :], 0.0)
            + jnp.where(hit_second, route_in[1:2, :], 0.0),
            axis=1,
            keepdims=True,
        )
        pick_buf[target] = pick
        return pick, weight

    bufs = (x_buf, c_buf)
    outs = (rows_out, cot_out)
    more = (rows_more, cot_more)

    def remote(source, target, sems, index, axis, other):
        return pltpu.make_async_remote_copy(
            src_ref=source,
            dst_ref=target,
            send_sem=sems.at[(0,) + index],
            recv_sem=sems.at[(1,) + index],
            device_id={axis: other},
            device_id_type=mesh_ids,
        )

    def z_copy(which, step):
        other = flipped(place, step, count)
        return remote(
            outs[which].at[other], bufs[which].at[place, me], z_sems, (which, step), "sp", other
        )

    def x_copy(which, step):
        ref = bufs[which].at[flipped(place, step, count), me]
        return remote(ref, ref, x_sems, (which, step), "tp", far)

    def direct_copy(which, step):
        other = flipped(place, step, count)
        return remote(
            more[which].at[step - 1], bufs[which].at[place, far], x_sems, (which, step), "sp", other
        )

    def d_copy(which, turn, step):
        ref = bufs[which].at[flipped(place, step, count), far if turn else me]
        return remote(ref, ref, d_sems, (which, turn, step), "tp", near)

    def near_copy(turn, step):
        origin = flipped(place, step, count)
        return remote(
            part_buf.at[origin, cross if turn else near],
            near_buf.at[origin, turn],
            near_sems,
            (turn, step),
            "tp",
            near,
        )

    def far_copy(step):
        origin = flipped(place, step, count)
        return remote(far_send.at[origin], far_buf.at[origin], far_sems, (step,), "tp", far)

    def back_copy(step):
        origin = flipped(place, step, count)
        return remote(back_send.at[origin], returned.at[place], back_sems, (step,), "sp", origin)

    def edge_copy(step):
        other = flipped(place, step, count)
        return remote(edge_send, edge_buf.at[place], edge_sems, (step,), "sp", other)

    def gather_copy(turn):
        if turn == 0:
            return remote(full_cot.at[me], full_cot.at[me], gather_sems, (0,), "tp", far)
        ref = full_cot.at[me if turn == 1 else far]
        return remote(ref, ref, gather_sems, (turn,), "tp", near)

    for load in loads[:early]:
        load.wait()
    pl.semaphore_wait(barrier, count + 1)

    def send_rows(step, carry):
        target = flipped(place, step, count)
        pick, weight = picks(target)
        rows_out[target] = plain_dot(pick, layer_buf[me]).astype(bf16)
        z_copy(0, step).start()
        cot_out[target] = (plain_dot(pick, cot_buf[me]) * weight).astype(bf16)
        z_copy(1, step).start()

        @pl.when(step <= direct_steps)
        def _():
            rows_more[step - 1] = plain_dot(pick, layer_buf[far]).astype(bf16)
            direct_copy(0, step).start()
            cot_more[step - 1] = (plain_dot(pick, cot_buf[far]) * weight).astype(bf16)
            direct_copy(1, step).start()

        return carry

    lax.fori_loop(1, count, send_rows, 0)
    pick, weight = picks(place)
    for p in range(pieces):
        x_buf[place, p] = plain_dot(pick, layer_buf[p]).astype(bf16)
        c_buf[place, p] = (plain_dot(pick, cot_buf[p]) * weight).astype(bf16)
    for load in loads[early:]:
        load.wait()

    def recurrence():
        rate = rates_in[me]
        rate_scale = decay_factor * (
            jnp.maximum(-rate, 0.0) + jnp.log1p(jnp.exp(-jnp.abs(rate)))
        )
        extra = extra_in[...]
        if heads % 8:
            extra = jnp.concatenate([extra, jnp.zeros((8 - heads % 8, tokens), f32)], axis=0)
        extra = extra.T
        for h in range(heads):
            cut = slice(h * head_width, (h + 1) * head_width)
            rows = rec_in[:, cut]
            rgate = jax.nn.sigmoid(plain_dot(rows, map_a_in[me * heads + h]))
            igate = jax.nn.sigmoid(plain_dot(rows, map_i_in[me * heads + h]))
            log_decay = -rate_scale[:, cut] * rgate + extra[:, h : h + 1]
            decay = jnp.exp(log_decay)
            scale = jnp.sqrt(one_minus_exp(2.0 * log_decay))
            state = decay * prev_in[:, cut] + scale * igate * rows.astype(f32)
            act, slope = gelu_pair(gate_in[:, cut].astype(f32))
            rgate_buf[:, cut] = rgate
            igate_buf[:, cut] = igate
            decay_buf[:, cut] = decay
            scale_buf[:, cut] = scale
            state_buf[:, cut] = state
            act_buf[:, cut] = act
            slope_buf[:, cut] = slope
            rec_out[:, cut] = (state * act).astype(bf16)
        return rate_scale

    rate_scale = recurrence()

    def arrive(step):
        for which in range(2):
            z_copy(which, step).wait_recv()

            @pl.when(step > direct_steps)
            def _():
                x_copy(which, step).start()

            d_copy(which, 0, step).start()

    def pass_on(step):
        for which in range(2):
            x_copy(which, step).wait_recv()
            d_copy(which, 1, step).start()
        for which in range(2):
            for turn in range(2):
                d_copy(which, turn, step).wait_recv()

    def compute(step):
        origin = flipped(place, step, count)
        width = w_gate.shape[2]
        gate_pre = jnp.zeros((cap, width), f32)
        up_pre = jnp.zeros((cap, width), f32)
        hidden_cot = jnp.zeros((cap, width), f32)
        for p in range(pieces):
            row_block = x_buf[origin, p]
            gate_pre += plain_dot(row_block, w_gate[p])
            up_pre += plain_dot(row_block, w_up[p])
            hidden_cot += columns_dot(c_buf[origin, p], w_down[:, p * piece : (p + 1) * piece])
        sigma = jax.nn.sigmoid(gate_pre)
        swish = gate_pre * sigma
        hidden_buf[origin] = (swish * up_pre).astype(bf16)
        gate_cot = (hidden_cot * up_pre * sigma * (1.0 + gate_pre * (1.0 - sigma))).astype(bf16)
        up_cot = (hidden_cot * swish).astype(bf16)
        gate_c[origin] = gate_cot
        up_c[origin] = up_cot
        for p in range(pieces):
            part_buf[origin, p] = (
                columns_dot(gate_cot, w_gate[p]) + columns_dot(up_cot, w_up[p])
            ).astype(bf16)
        for turn in range(2):
            near_copy(turn, step).start()

    def halve(step):
        origin = flipped(place, step, count)
        for turn in range(2):
            near_copy(turn, step).wait_recv()
        far_send[origin] = (
            part_buf[origin, far].astype(f32) + near_buf[origin, 1].astype(f32)
        ).astype(bf16)
        far_copy(step).start()

    def finish(step):
        origin = flipped(place, step, count)
        far_copy(step).wait_recv()
        total = (
            part_buf[origin, me].astype(f32)
            + near_buf[origin, 0].astype(f32)
            + far_buf[origin].astype(f32)
        ).astype(bf16)

        @pl.when(step == 0)
        def _():
            returned[place] = total

        @pl.when(step > 0)
        def _():
            back_send[origin] = total
            back_copy(step).start()

    def run(step, carry):
        @pl.when(step + 1 < count)
        def _():
            arrive(step + 1)

        @pl.when(step >= 1)
        def _():
            pass_on(step)

        compute(step)

        @pl.when(step >= 1)
        def _():
            finish(step - 1)

        halve(step)
        return carry

    lax.fori_loop(0, count, run, 0)

    width = w_gate.shape[2]
    tile = min(piece, 256)
    rows = count * cap

    def over_rows(left, right):
        if cap % 16 == 0:
            return rows_dot(left().reshape(rows, -1), right().reshape(rows, -1))
        total = rows_dot(left()[0], right()[0])
        for s in range(1, count):
            total = total + rows_dot(left()[s], right()[s])
        return total

    def gradients(p, carry):
        for t in range(piece // tile):
            spot = pl.ds(pl.multiple_of(p * piece + t * tile, tile), tile)
            cut = slice(t * tile, (t + 1) * tile)
            gate_grad[spot, :] = over_rows(lambda: x_buf[:, p, :, cut], lambda: gate_c[...])
            up_grad[spot, :] = over_rows(lambda: x_buf[:, p, :, cut], lambda: up_c[...])
            down_grad[:, spot] = over_rows(lambda: hidden_buf[...], lambda: c_buf[:, p, :, cut])
        return carry

    lax.fori_loop(0, half, gradients, 0)
    finish(count - 1)
    lax.fori_loop(half, pieces, gradients, 0)
    stores = [
        pltpu.make_async_copy(vmem, hbm, store_sems.at[i])
        for i, (vmem, hbm) in enumerate(
            [
                (gate_grad, gate_grad_out),
                (up_grad, up_grad_out),
                (down_grad, down_grad_out),
            ]
        )
    ]
    for store in stores:
        store.start()

    def add_slots(step, total):
        origin = flipped(place, step, count)
        back_copy(step).wait_recv()
        return total + rows_dot(pick_buf[origin], returned[origin])

    slots = rows_dot(pick_buf[place], returned[place])
    slots = lax.fori_loop(1, count, add_slots, slots)
    full_cot[me] = (cot_buf[me].astype(f32) + slots).astype(bf16)
    gather_copy(0).start()
    gather_copy(1).start()

    term_rows = piece * pieces // count
    per_piece = piece // term_rows

    def term_copy(block):
        return pltpu.make_async_remote_copy(
            src_ref=term_send.at[block],
            dst_ref=term_buf.at[place],
            send_sem=term_sems.at[0, block],
            recv_sem=term_sems.at[1, place],
            device_id={"sp": block},
            device_id_type=mesh_ids,
        )

    def arrival(source):
        return pltpu.make_async_remote_copy(
            src_ref=term_send.at[source],
            dst_ref=term_buf.at[source],
            send_sem=term_sems.at[0, source],
            recv_sem=term_sems.at[1, source],
            device_id={"sp": source},
            device_id_type=mesh_ids,
        )

    def use(p, start):
        block = full_cot[p]
        product = plain_dot(block, out_proj[p])
        if start:
            mix_buf[...] = product
        else:
            mix_buf[...] += product
        for j in range(per_piece):
            target = p * per_piece + j
            cut = slice(j * term_rows, (j + 1) * term_rows)
            term = rows_dot(full_cot[p, :, cut], rec_out[...]).astype(bf16) if (
                term_rows % 128 == 0
            ) else rows_dot(block, rec_out[...])[cut].astype(bf16)
            term_send[target] = term

            @pl.when(target != place)
            def _():
                term_copy(target).start()

            @pl.when(target == place)
            def _():
                term_buf[place] = term

    use(me, True)
    gather_copy(1).wait_recv()
    use(near, False)
    gather_copy(0).wait_recv()
    gather_copy(2).start()
    use(far, False)
    gather_copy(2).wait_recv()
    use(cross, False)

    for h in range(heads):
        cut = slice(h * head_width, (h + 1) * head_width)
        decay = decay_buf[:, cut]
        index = lax.broadcasted_iota(jnp.int32, decay.shape, 0)
        link = jnp.where(index < tokens - 1, pltpu.roll(decay, tokens - 1, 0), 1.0)
        product, total = scan_columns(link, mix_buf[:, cut] * act_buf[:, cut])
        product_buf[:, cut] = product
        local_buf[:, cut] = total
        edge_send[0:1, cut] = decay[0:1] * product[0:1]
        edge_send[1:2, cut] = decay[0:1] * total[0:1]
        edge_send[2:8, cut] = jnp.zeros((6, head_width), f32)

    def send_edge(step, carry):
        edge_copy(step).start()
        return carry

    lax.fori_loop(1, count, send_edge, 0)
    gate_input_out[...] = (mix_buf[...] * state_buf[...] * slope_buf[...]).astype(bf16)

    def wait_edge(step, carry):
        edge_copy(step).wait_recv()
        return carry

    lax.fori_loop(1, count, wait_edge, 0)
    edge_buf[place] = edge_send[...]

    def carry_on(turn, carry):
        source = count - 1 - turn
        step = edge_buf[source, 1:2] + edge_buf[source, 0:1] * carry
        return jnp.where(source > place, step, carry)

    carried = lax.fori_loop(0, count - 1, carry_on, jnp.zeros((1, channels), f32))
    for h in range(heads):
        cut = slice(h * head_width, (h + 1) * head_width)
        values_in = rec_in[:, cut].astype(f32)
        decay, scale = decay_buf[:, cut], scale_buf[:, cut]
        rgate, igate = rgate_buf[:, cut], igate_buf[:, cut]
        state_cot = local_buf[:, cut] + product_buf[:, cut] * carried[:, cut]
        log_cot = state_cot * (
            decay * prev_in[:, cut] - decay * decay / scale * igate * values_in
        )
        a_pre = (log_cot * -rate_scale[:, cut] * rgate * (1.0 - rgate)).astype(bf16)
        i_pre = (state_cot * scale * values_in * igate * (1.0 - igate)).astype(bf16)
        rec_grad_out[:, cut] = (
            state_cot * scale * igate
            + columns_dot(a_pre, map_a_in[me * heads + h])
            + columns_dot(i_pre, map_i_in[me * heads + h])
        ).astype(bf16)

    def wait_term(step, carry):
        arrival(flipped(place, step, count)).wait_recv()
        return carry

    lax.fori_loop(1, count, wait_term, 0)

    def sum_terms(source, total):
        return total + term_buf[source].astype(f32)

    proj_grad_out[...] = lax.fori_loop(
        1, count, sum_terms, term_buf[0].astype(f32)
    )

    def settle(step, carry):
        for turn in range(2):
            near_copy(turn, step).wait_send()
        far_copy(step).wait_send()
        return carry

    def settle_far(step, carry):
        for which in range(2):
            z_copy(which, step).wait_send()
            x_copy(which, step).wait_send()
            for turn in range(2):
                d_copy(which, turn, step).wait_send()
        back_copy(step).wait_send()
        edge_copy(step).wait_send()
        arrival(flipped(place, step, count)).wait_send()
        return carry

    lax.fori_loop(0, count, settle, 0)
    lax.fori_loop(1, count, settle_far, 0)
    for turn in range(3):
        gather_copy(turn).wait_send()
    for store in stores:
        store.wait()


def per_device(
    layer_input,
    out_cot,
    expert_ids,
    route_weight,
    w_gate,
    w_up,
    w_down,
    out_proj,
    rec_input,
    gate_input,
    prev_state,
    decay_param,
    extra_decay,
    gate_a_w,
    gate_i_w,
):
    count = lax.axis_size("sp")
    pieces = lax.axis_size("tp")
    local_experts, width, hidden_width = w_gate.shape
    tokens, channels = rec_input.shape
    top_count = expert_ids.shape[1]
    assert local_experts == 1 and top_count == 2 and pieces == 4
    cap = 5 * tokens * top_count // (4 * count)
    piece = width // pieces
    term_rows = width // count
    head_count, head_width = gate_a_w.shape[:2]
    vmem = pl.BlockSpec(memory_space=pltpu.VMEM)
    anywhere = pl.BlockSpec(memory_space=pl.ANY)

    def sems(*dims):
        return pltpu.SemaphoreType.DMA(dims)

    def buf(*dims, dtype=bf16):
        return pltpu.VMEM(dims, dtype)

    rec_bufs = [buf(tokens, channels, dtype=f32)] * 7
    grads = pl.pallas_call(
        step_kernel,
        in_specs=[
            anywhere,
            anywhere,
            vmem,
            vmem,
            anywhere,
            anywhere,
            anywhere,
            anywhere,
            vmem,
            vmem,
            vmem,
            vmem,
            vmem,
            vmem,
            vmem,
        ],
        out_specs=[anywhere, anywhere, anywhere, vmem, vmem, vmem],
        out_shape=[
            jax.ShapeDtypeStruct((width, hidden_width), f32),
            jax.ShapeDtypeStruct((width, hidden_width), f32),
            jax.ShapeDtypeStruct((hidden_width, width), f32),
            jax.ShapeDtypeStruct((term_rows, channels), f32),
            jax.ShapeDtypeStruct((tokens, channels), bf16),
            jax.ShapeDtypeStruct((tokens, channels), bf16),
        ],
        scratch_shapes=[
            buf(pieces, tokens, piece),
            buf(pieces, tokens, piece),
            buf(count, cap, tokens),
            buf(count, cap, piece),
            buf(count, cap, piece),
            buf(direct_steps, cap, piece),
            buf(direct_steps, cap, piece),
            buf(count, pieces, cap, piece),
            buf(count, pieces, cap, piece),
            buf(count, pieces, cap, piece),
            buf(count, 2, cap, piece),
            buf(count, cap, piece),
            buf(count, cap, piece),
            buf(count, cap, piece),
            buf(count, cap, piece),
            buf(count, cap, hidden_width),
            buf(count, cap, hidden_width),
            buf(count, cap, hidden_width),
            buf(pieces, piece, hidden_width),
            buf(pieces, piece, hidden_width),
            buf(hidden_width, width),
            buf(pieces, piece, channels),
            buf(width, hidden_width, dtype=f32),
            buf(width, hidden_width, dtype=f32),
            buf(hidden_width, width, dtype=f32),
            *rec_bufs,
            buf(tokens, channels),
            buf(pieces, tokens, piece),
            buf(tokens, channels, dtype=f32),
            buf(count, term_rows, channels),
            buf(count, term_rows, channels),
            buf(8, channels, dtype=f32),
            buf(count, 8, channels, dtype=f32),
            buf(tokens, channels, dtype=f32),
            buf(tokens, channels, dtype=f32),
            sems(2, 2, count),
            sems(2, 2, count),
            sems(2, 2, 2, count),
            sems(2, 2, count),
            sems(2, count),
            sems(2, count),
            sems(2, 3),
            sems(2, count),
            sems(2, count),
            sems(2 * pieces + 4),
            sems(3),
        ],
        compiler_params=pltpu.CompilerParams(
            collective_id=0, has_side_effects=True, vmem_limit_bytes=63 * 1024 * 1024
        ),
        cost_estimate=pl.CostEstimate(
            flops=18 * count * cap * width * hidden_width,
            bytes_accessed=40 * count * cap * piece,
            transcendentals=0,
        ),
    )(
        layer_input,
        out_cot,
        expert_ids.T,
        route_weight.T,
        w_gate.reshape(pieces, piece, hidden_width),
        w_up.reshape(pieces, piece, hidden_width),
        w_down[0],
        out_proj.reshape(pieces, piece, channels),
        rec_input,
        gate_input,
        prev_state,
        decay_param.reshape(pieces, 1, channels),
        extra_decay,
        gate_a_w,
        gate_i_w,
    )
    grad_gate, grad_up, grad_down, grad_out_proj, rec_input_grad, gate_input_grad = grads
    return (
        grad_gate[None],
        grad_up[None],
        grad_down[None],
        grad_out_proj,
        rec_input_grad,
        gate_input_grad,
    )


def solution(mesh):
    in_specs = (
        P("sp", None),
        P("sp", None),
        P("sp", None),
        P("sp", None),
        P("sp", None, "tp"),
        P("sp", None, "tp"),
        P("sp", "tp", None),
        P(None, "tp"),
        P("sp", "tp"),
        P("sp", "tp"),
        P("sp", "tp"),
        P(),
        P("tp", "sp"),
        P(),
        P(),
    )
    out_specs = (
        P("sp", None, "tp"),
        P("sp", None, "tp"),
        P("sp", "tp", None),
        P("sp", "tp"),
        P("sp", "tp"),
        P("sp", "tp"),
    )
    return jax.shard_map(
        per_device, mesh=mesh, in_specs=in_specs, out_specs=out_specs, check_vma=False
    )
```

```python
import functools

import jax
import jax.numpy as jnp
from jax import lax
from jax.experimental import pallas as pl
from jax.experimental.pallas import tpu as pltpu
from jax.sharding import PartitionSpec as P

gelu_scale = 0.7978845608028654
gelu_cubic = 0.044715
decay_factor = 8.0
direct_steps = 2
gather_parts = 2
mesh_ids = pl.DeviceIdType.MESH
f32 = jnp.float32
bf16 = jnp.bfloat16


def flipped(index, mask, count):
    result = index
    bit = 1
    while bit < count:
        own = (index // bit) % 2
        turn = (mask // bit) % 2
        result = result + bit * turn * (1 - 2 * own)
        bit *= 2
    return result


def plain_dot(left, right):
    return jnp.dot(left, right, preferred_element_type=f32)


def columns_dot(left, right):
    return lax.dot_general(left, right, (((1,), (1,)), ((), ())), preferred_element_type=f32)


def rows_dot(left, right):
    return lax.dot_general(left, right, (((0,), (0,)), ((), ())), preferred_element_type=f32)


def gelu_pair(values_in):
    inner = gelu_scale * (values_in + gelu_cubic * values_in * values_in * values_in)
    bend = jnp.tanh(inner)
    active = 0.5 * values_in * (1.0 + bend)
    slope = 0.5 * (1.0 + bend) + 0.5 * values_in * (1.0 - bend * bend) * gelu_scale * (
        1.0 + 3.0 * gelu_cubic * values_in * values_in
    )
    return (active, slope)


def one_minus_exp(value):
    series = value * (
        1.0
        + value * (0.5 + value * (1.0 / 6 + value * (1.0 / 24 + value * (1.0 / 120 + value / 720))))
    )
    return jnp.where(value > -0.25, -series, 1.0 - jnp.exp(value))


def scan_columns(link, total):
    rows, cols = link.shape
    row_index = lax.broadcasted_iota(jnp.int32, (rows, cols), 0)
    step = 1
    while step < rows:
        if step < 8:
            inside = row_index < rows - step
            later_link = jnp.where(inside, pltpu.roll(link, rows - step, 0), 1.0)
            later_total = jnp.where(inside, pltpu.roll(total, rows - step, 0), 0.0)
        else:
            later_link = jnp.concatenate([link[step:], jnp.ones((step, cols), f32)], axis=0)
            later_total = jnp.concatenate([total[step:], jnp.zeros((step, cols), f32)], axis=0)
        total = total + link * later_total
        link = link * later_link
        step *= 2
    return link, total


def step_kernel(*refs):
    (
        layer_in,
        cot_in,
        ids_in,
        route_in,
        w_gate_in,
        w_up_in,
        w_down_in,
        out_proj_in,
        rec_in,
        gate_in,
        prev_in,
        rates_in,
        extra_in,
        map_a_in,
        map_i_in,
        gate_grad_out,
        up_grad_out,
        down_grad_out,
        proj_grad_out,
        rec_grad_out,
        gate_input_out,
        layer_buf,
        cot_buf,
        pick_buf,
        rows_out,
        cot_out,
        rows_more,
        cot_more,
        x_buf,
        c_buf,
        part_buf,
        near_buf,
        far_send,
        far_buf,
        back_send,
        returned,
        gate_c,
        up_c,
        hidden_buf,
        w_gate,
        w_up,
        w_down,
        out_proj,
        gate_grad,
        up_grad,
        down_grad,
        decay_buf,
        act_buf,
        bend_buf,
        a_buf,
        i_buf,
        keep_buf,
        rec_out,
        full_cot,
        mix_buf,
        term_send,
        term_buf,
        edge_send,
        edge_buf,
        product_buf,
        local_buf,
        z_sems,
        x_sems,
        d_sems,
        near_sems,
        far_sems,
        back_sems,
        gather_sems,
        term_sems,
        edge_sems,
        load_sems,
        store_sems,
    ) = refs
    count, pieces, cap, piece = x_buf.shape
    tokens, channels = rec_in.shape
    head_width = map_a_in.shape[1]
    heads = channels // head_width
    place = lax.axis_index("sp")
    me = lax.axis_index("tp")
    half = pieces // 2
    far = lax.rem(me + half, pieces)
    near = flipped(me, 1, 2)
    cross = lax.rem(near + half, pieces)

    loads = []
    for p in range(pieces):
        cut = pl.ds(p * piece, piece)
        loads.append((layer_in.at[:, cut], layer_buf.at[p]))
        loads.append((cot_in.at[:, cut], cot_buf.at[p]))
    early = len(loads)
    loads += [(w_gate_in, w_gate), (w_up_in, w_up), (w_down_in, w_down), (out_proj_in, out_proj)]
    loads = [pltpu.make_async_copy(a, b, load_sems.at[i]) for i, (a, b) in enumerate(loads)]
    for load in loads:
        load.start()

    barrier = pltpu.get_barrier_semaphore()

    def greet(step, carry):
        pl.semaphore_signal(
            barrier, inc=1, device_id={"sp": flipped(place, step, count)}, device_id_type=mesh_ids
        )
        return carry

    lax.fori_loop(1, count, greet, 0)
    for other in (far, near):
        pl.semaphore_signal(barrier, inc=1, device_id={"tp": other}, device_id_type=mesh_ids)

    expert_index = lax.broadcasted_iota(jnp.int32, (count, tokens), 0)
    first = (expert_index == ids_in[0:1, :]).astype(f32)
    second = (expert_index == ids_in[1:2, :]).astype(f32)
    earlier = (
        lax.broadcasted_iota(jnp.int32, (tokens, tokens), 0)
        < lax.broadcasted_iota(jnp.int32, (tokens, tokens), 1)
    ).astype(f32)
    before = plain_dot((first + second).astype(bf16), earlier.astype(bf16))
    spots = before + (cap * expert_index).astype(f32)
    first_place = jnp.sum(first * spots, axis=0, keepdims=True)
    second_place = jnp.sum(second * spots, axis=0, keepdims=True)
    row_index = lax.broadcasted_iota(jnp.int32, (cap, tokens), 0)

    def picks(target):
        rows = (row_index + target * cap).astype(f32)
        hit_first = rows == first_place
        hit_second = rows == second_place
        pick = jnp.where(hit_first | hit_second, 1.0, 0.0).astype(bf16)
        weight = jnp.sum(
            jnp.where(hit_first, route_in[0:1, :], 0.0)
            + jnp.where(hit_second, route_in[1:2, :], 0.0),
            axis=1,
            keepdims=True,
        )
        pick_buf[target] = pick
        return pick, weight

    bufs = (x_buf, c_buf)
    outs = (rows_out, cot_out)
    more = (rows_more, cot_more)

    def remote(source, target, sems, index, axis, other):
        return pltpu.make_async_remote_copy(
            src_ref=source,
            dst_ref=target,
            send_sem=sems.at[(0,) + index],
            recv_sem=sems.at[(1,) + index],
            device_id={axis: other},
            device_id_type=mesh_ids,
        )

    def z_copy(which, step):
        other = flipped(place, step, count)
        return remote(
            outs[which].at[other], bufs[which].at[place, me], z_sems, (which, step), "sp", other
        )

    def x_copy(which, step):
        ref = bufs[which].at[flipped(place, step, count), me]
        return remote(ref, ref, x_sems, (which, step), "tp", far)

    def direct_copy(which, step):
        other = flipped(place, step, count)
        return remote(
            more[which].at[step - 1], bufs[which].at[place, far], x_sems, (which, step), "sp", other
        )

    def d_copy(which, turn, step):
        ref = bufs[which].at[flipped(place, step, count), far if turn else me]
        return remote(ref, ref, d_sems, (which, turn, step), "tp", near)

    def near_copy(turn, step):
        origin = flipped(place, step, count)
        return remote(
            part_buf.at[origin, cross if turn else near],
            near_buf.at[origin, turn],
            near_sems,
            (turn, step),
            "tp",
            near,
        )

    def far_copy(step):
        origin = flipped(place, step, count)
        return remote(far_send.at[origin], far_buf.at[origin], far_sems, (step,), "tp", far)

    def back_copy(step):
        origin = flipped(place, step, count)
        return remote(back_send.at[origin], returned.at[place], back_sems, (step,), "sp", origin)

    def edge_copy(step):
        other = flipped(place, step, count)
        return remote(edge_send, edge_buf.at[place], edge_sems, (step,), "sp", other)

    def gather_copy(turn, part):
        owner = far if turn == 2 else me
        ref = full_cot.at[owner * gather_parts + part]
        axis_end = near if turn else far
        return remote(ref, ref, gather_sems, (turn, part), "tp", axis_end)

    for load in loads[:early]:
        load.wait()
    pl.semaphore_wait(barrier, count + 1)

    def send_rows(step, carry):
        target = flipped(place, step, count)
        pick, weight = picks(target)
        rows_out[target] = plain_dot(pick, layer_buf[me]).astype(bf16)
        z_copy(0, step).start()
        cot_out[target] = (plain_dot(pick, cot_buf[me]) * weight).astype(bf16)
        z_copy(1, step).start()

        @pl.when(step <= direct_steps)
        def _():
            rows_more[step - 1] = plain_dot(pick, layer_buf[far]).astype(bf16)
            direct_copy(0, step).start()
            cot_more[step - 1] = (plain_dot(pick, cot_buf[far]) * weight).astype(bf16)
            direct_copy(1, step).start()

        return carry

    lax.fori_loop(1, count, send_rows, 0)
    pick, weight = picks(place)
    for p in range(pieces):
        x_buf[place, p] = plain_dot(pick, layer_buf[p]).astype(bf16)
        c_buf[place, p] = (plain_dot(pick, cot_buf[p]) * weight).astype(bf16)
    for load in loads[early:]:
        load.wait()

    def recurrence():
        rate = rates_in[me]
        rate_scale = decay_factor * (
            jnp.maximum(-rate, 0.0) + jnp.log1p(jnp.exp(-jnp.abs(rate)))
        )
        extra = extra_in[...]
        if heads % 8:
            extra = jnp.concatenate([extra, jnp.zeros((8 - heads % 8, tokens), f32)], axis=0)
        extra = extra.T
        for h in range(heads):
            cut = slice(h * head_width, (h + 1) * head_width)
            rows = rec_in[:, cut]
            rgate = jax.nn.sigmoid(plain_dot(rows, map_a_in[me * heads + h]))
            igate = jax.nn.sigmoid(plain_dot(rows, map_i_in[me * heads + h]))
            log_decay = -rate_scale[:, cut] * rgate + extra[:, h : h + 1]
            decay = jnp.exp(log_decay)
            scale = jnp.sqrt(one_minus_exp(2.0 * log_decay))
            state = decay * prev_in[:, cut] + scale * igate * rows.astype(f32)
            act, slope = gelu_pair(gate_in[:, cut].astype(f32))
            decay_buf[:, cut] = decay
            act_buf[:, cut] = act
            bend_buf[:, cut] = state * slope
            rec_out[:, cut] = (state * act).astype(bf16)
            values_in = rows.astype(f32)
            log_part = decay * prev_in[:, cut] - decay * decay / scale * igate * values_in
            a_buf[:, cut] = log_part * -rate_scale[:, cut] * rgate * (1.0 - rgate)
            i_buf[:, cut] = scale * values_in * igate * (1.0 - igate)
            keep_buf[:, cut] = scale * igate

    recurrence()

    def arrive(step):
        for which in range(2):
            z_copy(which, step).wait_recv()

            @pl.when(step > direct_steps)
            def _():
                x_copy(which, step).start()

            d_copy(which, 0, step).start()

    def pass_on(step):
        for which in range(2):
            x_copy(which, step).wait_recv()
            d_copy(which, 1, step).start()
        for which in range(2):
            for turn in range(2):
                d_copy(which, turn, step).wait_recv()

    def compute(step):
        origin = flipped(place, step, count)
        width = w_gate.shape[2]
        gate_pre = jnp.zeros((cap, width), f32)
        up_pre = jnp.zeros((cap, width), f32)
        hidden_cot = jnp.zeros((cap, width), f32)
        for p in range(pieces):
            row_block = x_buf[origin, p]
            gate_pre += plain_dot(row_block, w_gate[p])
            up_pre += plain_dot(row_block, w_up[p])
            hidden_cot += columns_dot(c_buf[origin, p], w_down[:, p * piece : (p + 1) * piece])
        sigma = jax.nn.sigmoid(gate_pre)
        swish = gate_pre * sigma
        hidden_buf[origin] = (swish * up_pre).astype(bf16)
        gate_cot = (hidden_cot * up_pre * sigma * (1.0 + gate_pre * (1.0 - sigma))).astype(bf16)
        up_cot = (hidden_cot * swish).astype(bf16)
        gate_c[origin] = gate_cot
        up_c[origin] = up_cot
        for p in range(pieces):
            part_buf[origin, p] = (
                columns_dot(gate_cot, w_gate[p]) + columns_dot(up_cot, w_up[p])
            ).astype(bf16)
        for turn in range(2):
            near_copy(turn, step).start()

    def halve(step):
        origin = flipped(place, step, count)
        for turn in range(2):
            near_copy(turn, step).wait_recv()
        far_send[origin] = (
            part_buf[origin, far].astype(f32) + near_buf[origin, 1].astype(f32)
        ).astype(bf16)
        far_copy(step).start()

    def finish(step):
        origin = flipped(place, step, count)
        far_copy(step).wait_recv()
        total = (
            part_buf[origin, me].astype(f32)
            + near_buf[origin, 0].astype(f32)
            + far_buf[origin].astype(f32)
        ).astype(bf16)

        @pl.when(step == 0)
        def _():
            returned[place] = total

        @pl.when(step > 0)
        def _():
            back_send[origin] = total
            back_copy(step).start()

    def run(step, carry):
        @pl.when(step + 1 < count)
        def _():
            arrive(step + 1)

        @pl.when(step >= 1)
        def _():
            pass_on(step)

        compute(step)

        @pl.when(step >= 1)
        def _():
            finish(step - 1)

        halve(step)
        return carry

    lax.fori_loop(0, count, run, 0)

    width = w_gate.shape[2]
    tile = min(piece, 256)
    rows = count * cap

    def over_rows(left, right):
        if cap % 16 == 0:
            return rows_dot(left().reshape(rows, -1), right().reshape(rows, -1))
        total = rows_dot(left()[0], right()[0])
        for s in range(1, count):
            total = total + rows_dot(left()[s], right()[s])
        return total

    def gradients(p, carry):
        for t in range(piece // tile):
            spot = pl.ds(pl.multiple_of(p * piece + t * tile, tile), tile)
            cut = slice(t * tile, (t + 1) * tile)
            gate_grad[spot, :] = over_rows(lambda: x_buf[:, p, :, cut], lambda: gate_c[...])
            up_grad[spot, :] = over_rows(lambda: x_buf[:, p, :, cut], lambda: up_c[...])
            down_grad[:, spot] = over_rows(lambda: hidden_buf[...], lambda: c_buf[:, p, :, cut])
        return carry

    lax.fori_loop(0, half, gradients, 0)
    finish(count - 1)
    lax.fori_loop(half, pieces, gradients, 0)
    stores = [
        pltpu.make_async_copy(vmem, hbm, store_sems.at[i])
        for i, (vmem, hbm) in enumerate(
            [
                (gate_grad, gate_grad_out),
                (up_grad, up_grad_out),
                (down_grad, down_grad_out),
            ]
        )
    ]
    for store in stores:
        store.start()

    def add_slots(step, total):
        origin = flipped(place, step, count)
        back_copy(step).wait_recv()
        return total + rows_dot(pick_buf[origin], returned[origin])

    slots = rows_dot(pick_buf[place], returned[place])
    slots = lax.fori_loop(1, count, add_slots, slots)
    chunk = piece // gather_parts
    for part in range(gather_parts):
        cut = slice(part * chunk, (part + 1) * chunk)
        full_cot[me * gather_parts + part] = (
            cot_buf[me, :, cut].astype(f32) + slots[:, cut]
        ).astype(bf16)
        gather_copy(0, part).start()
    for part in range(gather_parts):
        gather_copy(1, part).start()

    term_rows = piece * pieces // count
    per_chunk = chunk // term_rows

    def term_copy(block):
        return pltpu.make_async_remote_copy(
            src_ref=term_send.at[block],
            dst_ref=term_buf.at[place],
            send_sem=term_sems.at[0, block],
            recv_sem=term_sems.at[1, place],
            device_id={"sp": block},
            device_id_type=mesh_ids,
        )

    def arrival(source):
        return pltpu.make_async_remote_copy(
            src_ref=term_send.at[source],
            dst_ref=term_buf.at[source],
            send_sem=term_sems.at[0, source],
            recv_sem=term_sems.at[1, source],
            device_id={"sp": source},
            device_id_type=mesh_ids,
        )

    def use(p, part, start=False):
        spot = p * gather_parts + part
        block = full_cot[spot]
        terms = rows_dot(block, rec_out[...]).astype(bf16)
        for j in range(per_chunk):
            target = spot * per_chunk + j
            term_send[target] = terms[j * term_rows : (j + 1) * term_rows]

            @pl.when(target != place)
            def _():
                term_copy(target).start()

            @pl.when(target == place)
            def _():
                term_buf[place] = term_send[target]

        product = plain_dot(block, out_proj[spot])
        if start:
            mix_buf[...] = product
        else:
            mix_buf[...] += product

    for part in range(gather_parts):
        use(me, part, part == 0)
    for part in range(gather_parts):
        gather_copy(1, part).wait_recv()
        use(near, part)
    for part in range(gather_parts):
        gather_copy(0, part).wait_recv()
        gather_copy(2, part).start()
        use(far, part)
        gather_copy(2, part).wait_recv()
        use(cross, part)

    for h in range(heads):
        cut = slice(h * head_width, (h + 1) * head_width)
        decay = decay_buf[:, cut]
        index = lax.broadcasted_iota(jnp.int32, decay.shape, 0)
        link = jnp.where(index < tokens - 1, pltpu.roll(decay, tokens - 1, 0), 1.0)
        product, total = scan_columns(link, mix_buf[:, cut] * act_buf[:, cut])
        product_buf[:, cut] = product
        local_buf[:, cut] = total
        edge_send[0:1, cut] = decay[0:1] * product[0:1]
        edge_send[1:2, cut] = decay[0:1] * total[0:1]
        edge_send[2:8, cut] = jnp.zeros((6, head_width), f32)

    def send_edge(step, carry):
        edge_copy(step).start()
        return carry

    lax.fori_loop(1, count, send_edge, 0)
    gate_input_out[...] = (mix_buf[...] * bend_buf[...]).astype(bf16)

    def wait_edge(step, carry):
        edge_copy(step).wait_recv()
        return carry

    lax.fori_loop(1, count, wait_edge, 0)
    edge_buf[place] = edge_send[...]

    def carry_on(turn, carry):
        source = count - 1 - turn
        step = edge_buf[source, 1:2] + edge_buf[source, 0:1] * carry
        return jnp.where(source > place, step, carry)

    carried = lax.fori_loop(0, count - 1, carry_on, jnp.zeros((1, channels), f32))
    for h in range(heads):
        cut = slice(h * head_width, (h + 1) * head_width)
        state_cot = local_buf[:, cut] + product_buf[:, cut] * carried[:, cut]
        a_pre = (state_cot * a_buf[:, cut]).astype(bf16)
        i_pre = (state_cot * i_buf[:, cut]).astype(bf16)
        rec_grad_out[:, cut] = (
            state_cot * keep_buf[:, cut]
            + columns_dot(a_pre, map_a_in[me * heads + h])
            + columns_dot(i_pre, map_i_in[me * heads + h])
        ).astype(bf16)

    def wait_term(step, carry):
        arrival(flipped(place, step, count)).wait_recv()
        return carry

    lax.fori_loop(1, count, wait_term, 0)

    def sum_terms(source, total):
        return total + term_buf[source].astype(f32)

    proj_grad_out[...] = lax.fori_loop(
        1, count, sum_terms, term_buf[0].astype(f32)
    )

    def settle(step, carry):
        for turn in range(2):
            near_copy(turn, step).wait_send()
        far_copy(step).wait_send()
        return carry

    def settle_far(step, carry):
        for which in range(2):
            z_copy(which, step).wait_send()
            x_copy(which, step).wait_send()
            for turn in range(2):
                d_copy(which, turn, step).wait_send()
        back_copy(step).wait_send()
        edge_copy(step).wait_send()
        arrival(flipped(place, step, count)).wait_send()
        return carry

    lax.fori_loop(0, count, settle, 0)
    lax.fori_loop(1, count, settle_far, 0)
    for turn in range(3):
        for part in range(gather_parts):
            gather_copy(turn, part).wait_send()
    for store in stores:
        store.wait()


def result_kernel(cuts, *refs):
    arrays = len(cuts)
    sources, targets = refs[:arrays], refs[arrays : 2 * arrays]
    holds, (in_sems, out_sems) = refs[2 * arrays : 3 * arrays], refs[3 * arrays :]
    moves = []
    for which, parts in enumerate(cuts):
        rows = holds[which].shape[0] // parts
        for part in range(parts):
            spot = pl.ds(part * rows, rows)
            number = len(moves)
            moves.append(
                (
                    pltpu.make_async_copy(
                        sources[which].at[spot], holds[which].at[spot], in_sems.at[number]
                    ),
                    pltpu.make_async_copy(
                        holds[which].at[spot], targets[which].at[spot], out_sems.at[number]
                    ),
                )
            )
    for read, _ in moves:
        read.start()
    for read, write in moves:
        read.wait()
        write.start()
    for _, write in moves:
        write.wait()


def results_of(arrays):
    cuts = [max(1, min(8, a.size * a.dtype.itemsize // (512 * 1024))) for a in arrays]
    anywhere = pl.BlockSpec(memory_space=pl.ANY)
    return pl.pallas_call(
        functools.partial(result_kernel, cuts),
        in_specs=[anywhere] * len(arrays),
        out_specs=[anywhere] * len(arrays),
        out_shape=[jax.ShapeDtypeStruct(a.shape, a.dtype) for a in arrays],
        scratch_shapes=[pltpu.VMEM(a.shape, a.dtype) for a in arrays]
        + [pltpu.SemaphoreType.DMA((sum(cuts),))] * 2,
    )(*arrays)


def per_device(
    layer_input,
    out_cot,
    expert_ids,
    route_weight,
    w_gate,
    w_up,
    w_down,
    out_proj,
    rec_input,
    gate_input,
    prev_state,
    decay_param,
    extra_decay,
    gate_a_w,
    gate_i_w,
):
    count = lax.axis_size("sp")
    pieces = lax.axis_size("tp")
    local_experts, width, hidden_width = w_gate.shape
    tokens, channels = rec_input.shape
    top_count = expert_ids.shape[1]
    assert local_experts == 1 and top_count == 2 and pieces == 4
    cap = 5 * tokens * top_count // (4 * count)
    piece = width // pieces
    term_rows = width // count
    head_count, head_width = gate_a_w.shape[:2]
    vmem = pl.BlockSpec(memory_space=pltpu.VMEM)
    anywhere = pl.BlockSpec(memory_space=pl.ANY)

    def sems(*dims):
        return pltpu.SemaphoreType.DMA(dims)

    def buf(*dims, dtype=bf16):
        return pltpu.VMEM(dims, dtype)

    rec_bufs = [buf(tokens, channels, dtype=f32)] * 6
    grads = pl.pallas_call(
        step_kernel,
        in_specs=[
            anywhere,
            anywhere,
            vmem,
            vmem,
            anywhere,
            anywhere,
            anywhere,
            anywhere,
            vmem,
            vmem,
            vmem,
            vmem,
            vmem,
            vmem,
            vmem,
        ],
        out_specs=[anywhere, anywhere, anywhere, vmem, vmem, vmem],
        out_shape=[
            jax.ShapeDtypeStruct((width, hidden_width), f32),
            jax.ShapeDtypeStruct((width, hidden_width), f32),
            jax.ShapeDtypeStruct((hidden_width, width), f32),
            jax.ShapeDtypeStruct((term_rows, channels), f32),
            jax.ShapeDtypeStruct((tokens, channels), bf16),
            jax.ShapeDtypeStruct((tokens, channels), bf16),
        ],
        scratch_shapes=[
            buf(pieces, tokens, piece),
            buf(pieces, tokens, piece),
            buf(count, cap, tokens),
            buf(count, cap, piece),
            buf(count, cap, piece),
            buf(direct_steps, cap, piece),
            buf(direct_steps, cap, piece),
            buf(count, pieces, cap, piece),
            buf(count, pieces, cap, piece),
            buf(count, pieces, cap, piece),
            buf(count, 2, cap, piece),
            buf(count, cap, piece),
            buf(count, cap, piece),
            buf(count, cap, piece),
            buf(count, cap, piece),
            buf(count, cap, hidden_width),
            buf(count, cap, hidden_width),
            buf(count, cap, hidden_width),
            buf(pieces, piece, hidden_width),
            buf(pieces, piece, hidden_width),
            buf(hidden_width, width),
            buf(pieces * gather_parts, piece // gather_parts, channels),
            buf(width, hidden_width, dtype=f32),
            buf(width, hidden_width, dtype=f32),
            buf(hidden_width, width, dtype=f32),
            *rec_bufs,
            buf(tokens, channels),
            buf(pieces * gather_parts, tokens, piece // gather_parts),
            buf(tokens, channels, dtype=f32),
            buf(count, term_rows, channels),
            buf(count, term_rows, channels),
            buf(8, channels, dtype=f32),
            buf(count, 8, channels, dtype=f32),
            buf(tokens, channels, dtype=f32),
            buf(tokens, channels, dtype=f32),
            sems(2, 2, count),
            sems(2, 2, count),
            sems(2, 2, 2, count),
            sems(2, 2, count),
            sems(2, count),
            sems(2, count),
            sems(2, 3, gather_parts),
            sems(2, count),
            sems(2, count),
            sems(2 * pieces + 4),
            sems(3),
        ],
        compiler_params=pltpu.CompilerParams(
            collective_id=0, has_side_effects=True, vmem_limit_bytes=63 * 1024 * 1024
        ),
        cost_estimate=pl.CostEstimate(
            flops=18 * count * cap * width * hidden_width,
            bytes_accessed=40 * count * cap * piece,
            transcendentals=0,
        ),
    )(
        layer_input,
        out_cot,
        expert_ids.T,
        route_weight.T,
        w_gate.reshape(pieces, piece, hidden_width),
        w_up.reshape(pieces, piece, hidden_width),
        w_down[0],
        out_proj.reshape(pieces * gather_parts, piece // gather_parts, channels),
        rec_input,
        gate_input,
        prev_state,
        decay_param.reshape(pieces, 1, channels),
        extra_decay,
        gate_a_w,
        gate_i_w,
    )
    grad_gate, grad_up, grad_down, grad_out_proj, rec_input_grad, gate_input_grad = results_of(grads)
    return (
        grad_gate[None],
        grad_up[None],
        grad_down[None],
        grad_out_proj,
        rec_input_grad,
        gate_input_grad,
    )


def solution(mesh):
    in_specs = (
        P("sp", None),
        P("sp", None),
        P("sp", None),
        P("sp", None),
        P("sp", None, "tp"),
        P("sp", None, "tp"),
        P("sp", "tp", None),
        P(None, "tp"),
        P("sp", "tp"),
        P("sp", "tp"),
        P("sp", "tp"),
        P(),
        P("tp", "sp"),
        P(),
        P(),
    )
    out_specs = (
        P("sp", None, "tp"),
        P("sp", None, "tp"),
        P("sp", "tp", None),
        P("sp", "tp"),
        P("sp", "tp"),
        P("sp", "tp"),
    )
    return jax.shard_map(
        per_device, mesh=mesh, in_specs=in_specs, out_specs=out_specs, check_vma=False
    )
```
